512 devices in a mesh: sp: 64 (over z, y), fs: 4 (over x), tp: 2 (over core).
Axes of the slice: x: 4, y: 8, z: 8, core: 2. Of those that a mesh axis runs over, the one named last changes fastest.
Arguments:
- tokens: bfloat16 [16384, 2048], P(('sp', 'fs', 'tp')), may hold values from -6 to 6
- norm_gain: float32 [2048], replicated, may hold values from 0.1 to 1.9
- w_query: bfloat16 [2048, 2048], P(None, ('fs', 'tp')), may hold values from -0.9722718 to 0.9722718
- w_key: bfloat16 [2048, 512], P(None, 'fs'), may hold values from -0.77339804 to 0.77339804
- w_value: bfloat16 [2048, 512], P(None, 'fs'), may hold values from -0.125 to 0.125
- w_conv_value: bfloat16 [2048, 1024], P(None, ('fs', 'tp')), may hold values from -0.125 to 0.125
- w_conv_pre: bfloat16 [2048, 1024], P(None, ('fs', 'tp')), may hold values from -0.125 to 0.125
- w_conv_post: bfloat16 [2048, 1024], P(None, ('fs', 'tp')), may hold values from -0.125 to 0.125
- conv_taps: bfloat16 [3, 1024], replicated, may hold values from -3.5 to 3.5
- log_gate_cache: float32 [16, 16384], replicated, may hold values from -987 to 0, as said below
- w_out_conv: bfloat16 [1024, 2048], P(('fs', 'tp')), may hold values from -0.125 to 0.125
- w_out_attn: bfloat16 [2048, 2048], P(('fs', 'tp')), may hold values from -0.375 to 0.375
Outputs:
- mixed: bfloat16 [16384, 2048], P(('sp', 'fs', 'tp'))
The draws below stay inside these ranges and needn't reach their ends.
Inputs may be any that keep to these rules, and one draw needn't show every extreme that they name: `log_gate_cache`: each row is a cumulative sum over positions of log forget gates, none of them positive.
All inputs are finite; a program needn't handle non-finite values.
Results may differ from the reference program's by a relative error of at most 0.014.
The reference program's roundings to bfloat16 on the way count: a program that leaves them out, or rounds other values in their place, can miss the bound.
Values may be sent and summed in bfloat16 or wider, within the bound.
A program may use at most 64 MiB of HBM per device.

```python
import math
import jax
import jax.numpy as jnp
from jax import lax

D = 2048
QUERY_HEAD_COUNT = 16
KV_HEADS = 4
HEAD_DIM = 128
CHANNELS = 1024
KERNEL = 3
TOK_DEV = 256
SEQUENCE_LENGTH = 16384
N_FS = 4
N_TP = 2


def draw_w_query(key, part):
    entries = jnp.clip(jax.random.normal(jax.random.fold_in(key, 11), (D, QUERY_HEAD_COUNT * HEAD_DIM), jnp.float32), -6.0, 6.0) * (2.5 * D ** (-0.5))
    return entries.astype(jnp.bfloat16)


def draw_w_key(key, part):
    entries = jnp.clip(jax.random.normal(jax.random.fold_in(key, 13), (D, KV_HEADS * HEAD_DIM), jnp.float32), -6.0, 6.0) * D ** (-0.5)
    return entries.astype(jnp.bfloat16)


def draw_log_gate_cache(key, part):
    random_subseeds = jax.random.split(jax.random.fold_in(key, 23), 5)
    head_order = jax.random.permutation(random_subseeds[0], QUERY_HEAD_COUNT)
    fast_count = QUERY_HEAD_COUNT // 2
    fast_heads = head_order < fast_count
    block_count = SEQUENCE_LENGTH // TOK_DEV
    block_rate = jnp.exp(jax.random.uniform(random_subseeds[1], (QUERY_HEAD_COUNT, block_count), jnp.float32, -math.log(2.0), math.log(2.0)))
    jitter = jax.random.uniform(random_subseeds[2], (QUERY_HEAD_COUNT, SEQUENCE_LENGTH), jnp.float32, 0.5, 1.5)
    increment_frequency = jnp.repeat(block_rate, TOK_DEV, axis=1) * jitter
    baseline_frequency = jnp.where(fast_heads[:, None], 1.0 / min(50, TOK_DEV), 0.5 / SEQUENCE_LENGTH)
    spike_position = jax.random.randint(random_subseeds[3], (QUERY_HEAD_COUNT, 3), 0, SEQUENCE_LENGTH)
    spike_length = jax.random.uniform(random_subseeds[4], (QUERY_HEAD_COUNT, 3), jnp.float32, math.log(0.5), math.log(0.8))
    sequence_places = jnp.arange(SEQUENCE_LENGTH, dtype=jnp.int32)
    spike_events = jnp.sum(jnp.where(sequence_places[None, None, :] == spike_position[:, :, None], spike_length[:, :, None], 0.0), axis=1)
    return jnp.cumsum(spike_events - baseline_frequency * increment_frequency, axis=1)


def block_levels(own_key, dims, cuts, least, top_value):
    loudness = 1.0
    for dim, shards_of in cuts:
        heights = jax.random.uniform(jax.random.fold_in(jax.random.fold_in(own_key, 6), dim), (shards_of,), jnp.float32, least / len(cuts), top_value / len(cuts))
        loudness = loudness * jnp.repeat(jnp.exp(heights), dims[dim] // shards_of).reshape((-1,) + (1,) * (len(dims) - 1 - dim))
    return loudness


def gaussian(own_key, extent, scale, limit, pieces=(), kind=jnp.bfloat16):
    result = jax.random.normal(own_key, extent, jnp.float32) * scale
    if len(pieces) > 0:
        result = block_levels(own_key, extent, pieces, -0.22, 0.18) * result
    return jnp.clip(result, min=-limit, max=limit).astype(kind)


def setup_inputs(seed: int = 0) -> dict:
    arg_keys = jax.random.split(jax.random.key(seed), 13)
    return {
        "tokens": gaussian(arg_keys[0], (SEQUENCE_LENGTH, D), 1.0, 6.0, ((0, 512),)),
        "norm_gain": jnp.clip(1.0 + 0.18 * jax.random.normal(arg_keys[1], (D,), jnp.float32), 0.1, 1.9),
        "w_query": draw_w_query(jax.random.fold_in(arg_keys[12], 71), 0),
        "w_key": draw_w_key(jax.random.fold_in(arg_keys[12], 71), 0),
        "w_value": gaussian(arg_keys[4], (D, KV_HEADS * HEAD_DIM), D ** -0.5, 0.125, ((1, 4),)),
        "w_conv_value": gaussian(arg_keys[5], (D, CHANNELS), D ** -0.5, 0.125, ((1, 8),)),
        "w_conv_pre": gaussian(arg_keys[6], (D, CHANNELS), D ** -0.5, 0.125, ((1, 8),)),
        "w_conv_post": gaussian(arg_keys[7], (D, CHANNELS), D ** -0.5, 0.125, ((1, 8),)),
        "conv_taps": gaussian(arg_keys[8], (KERNEL, CHANNELS), KERNEL ** -0.5, 3.5),
        "log_gate_cache": draw_log_gate_cache(jax.random.fold_in(arg_keys[12], 71), 0),
        "w_out_conv": gaussian(arg_keys[10], (CHANNELS, D), (2 * CHANNELS) ** -0.5, 0.125, ((0, 8),)),
        "w_out_attn": gaussian(arg_keys[11], (QUERY_HEAD_COUNT * HEAD_DIM, D), (QUERY_HEAD_COUNT * HEAD_DIM // 8) ** -0.5, 0.375, ((0, 8),)),
    }


epsilon = 1e-06
masked_score = -1e+30

def attend_head(inputs):
    queries, keys, values, head_gates = inputs
    span = 512 if SEQUENCE_LENGTH % 512 == 0 else SEQUENCE_LENGTH
    blocks = SEQUENCE_LENGTH // span
    score_scale = HEAD_DIM ** (-0.5)
    query_blocks = queries.reshape(blocks, span, HEAD_DIM)
    gate_blocks = head_gates.reshape(blocks, span)

    def one_block(block_inputs):
        query_rows, gate_rows, block_index = block_inputs
        row_positions = block_index * span + jnp.arange(span, dtype=jnp.int32)

        def absorb(key_index, carry):
            running_max, running_sum, weighted = carry
            key_start = (key_index * span).astype(jnp.int32)
            key_rows = lax.dynamic_slice_in_dim(keys, key_start, span, 0)
            value_rows = lax.dynamic_slice_in_dim(values, key_start, span, 0)
            gate_keys = lax.dynamic_slice_in_dim(head_gates, key_start, span, 0)
            scores = jnp.dot(query_rows, key_rows.T, preferred_element_type=jnp.float32) * score_scale
            scores = scores + gate_rows[:, None] - gate_keys[None, :]
            key_positions = key_start + jnp.arange(span, dtype=jnp.int32)
            scores = jnp.where(row_positions[:, None] >= key_positions[None, :], scores, masked_score)
            new_max = jnp.maximum(running_max, lax.optimization_barrier(jnp.max(scores, axis=1)))
            rescale = jnp.exp(running_max - new_max)
            weights = jnp.exp(scores - new_max[:, None])
            running_sum = running_sum * rescale + lax.optimization_barrier(jnp.sum(weights, axis=1))
            weighted = weighted * rescale[:, None] + jnp.dot(weights.astype(jnp.bfloat16), value_rows, preferred_element_type=jnp.float32)
            return (new_max, running_sum, weighted)
        initial = (jnp.full((span,), masked_score, jnp.float32), jnp.zeros((span,), jnp.float32), jnp.zeros((span, HEAD_DIM), jnp.float32))
        final = lax.fori_loop(0, block_index + 1, absorb, initial)
        return (final[2] / final[1][:, None]).astype(jnp.bfloat16)
    outputs = lax.map(one_block, (query_blocks, gate_blocks, jnp.arange(blocks, dtype=jnp.int32)))
    return outputs.reshape(SEQUENCE_LENGTH, HEAD_DIM)

def reference(tokens, norm_gain, w_query, w_key, w_value, w_conv_value, w_conv_pre, w_conv_post, conv_taps, log_gate_cache, w_out_conv, w_out_attn):
    float_rows = tokens.astype(jnp.float32)
    normed = (float_rows * lax.rsqrt(lax.optimization_barrier(jnp.mean(float_rows * float_rows, axis=1, keepdims=True)) + epsilon) * norm_gain).astype(jnp.bfloat16)

    def project(weight):
        return jnp.dot(normed, weight, preferred_element_type=jnp.float32).astype(jnp.bfloat16)
    post_gate = project(w_conv_post)
    pre_gate = project(w_conv_pre)
    conv_value = project(w_conv_value)
    queries = project(w_query)
    keys = project(w_key)
    values = project(w_value)
    mixed_in = (pre_gate.astype(jnp.float32) * conv_value.astype(jnp.float32)).astype(jnp.bfloat16)
    padded = jnp.concatenate([jnp.zeros((KERNEL - 1, CHANNELS), jnp.bfloat16), mixed_in], axis=0).astype(jnp.float32)
    tap_weights = conv_taps.astype(jnp.float32)
    conv_sum = tap_weights[0] * padded[0:SEQUENCE_LENGTH]
    for offset in range(1, KERNEL):
        conv_sum = conv_sum + tap_weights[offset] * padded[offset:offset + SEQUENCE_LENGTH]
    conv_out = (post_gate.astype(jnp.float32) * conv_sum).astype(jnp.bfloat16)
    query_heads = queries.reshape(SEQUENCE_LENGTH, QUERY_HEAD_COUNT, HEAD_DIM).transpose(1, 0, 2)
    key_heads = jnp.repeat(keys.reshape(SEQUENCE_LENGTH, KV_HEADS, HEAD_DIM).transpose(1, 0, 2), QUERY_HEAD_COUNT // KV_HEADS, axis=0)
    value_heads = jnp.repeat(values.reshape(SEQUENCE_LENGTH, KV_HEADS, HEAD_DIM).transpose(1, 0, 2), QUERY_HEAD_COUNT // KV_HEADS, axis=0)
    attn_heads = lax.map(attend_head, (query_heads, key_heads, value_heads, log_gate_cache))
    attn_out = attn_heads.transpose(1, 0, 2).reshape(SEQUENCE_LENGTH, QUERY_HEAD_COUNT * HEAD_DIM)
    groups = N_FS * N_TP
    conv_width = CHANNELS // groups
    head_width = QUERY_HEAD_COUNT * HEAD_DIM // groups
    mixed = jnp.zeros((SEQUENCE_LENGTH, D), jnp.float32)
    for group in range(groups):
        partial_sum = jnp.dot(conv_out[:, group * conv_width:(group + 1) * conv_width], w_out_conv[group * conv_width:(group + 1) * conv_width], preferred_element_type=jnp.float32)
        partial_sum = partial_sum + jnp.dot(attn_out[:, group * head_width:(group + 1) * head_width], w_out_attn[group * head_width:(group + 1) * head_width], preferred_element_type=jnp.float32)
        mixed = mixed + lax.optimization_barrier(partial_sum.astype(jnp.bfloat16)).astype(jnp.float32)
    return mixed.astype(jnp.bfloat16)
```

```python
import functools
import math

import jax
import jax.numpy as jnp
from jax import lax
from jax.experimental import pallas as pl
from jax.experimental.pallas import tpu as pltpu
from jax.sharding import PartitionSpec as P

epsilon = 1e-06
masked_score = -1e30
MESH = pl.DeviceIdType.MESH
RING = 8


def in_order(tiles, dim):
    shape = list(tiles.shape[1:])
    shape[dim] *= tiles.shape[0]
    return jnp.moveaxis(tiles, 0, dim).reshape(shape)


def sent_to_all(value, axis):
    count = lax.axis_size(axis)
    return lax.all_to_all(
        jnp.broadcast_to(value[None], (count, *value.shape)), axis, 0, 0, tiled=True
    )


def gather_directly(value, axis, dim):
    return in_order(sent_to_all(value, axis), dim)


def passed_along(block, axis, distance):
    devices = range(lax.axis_size(axis))
    route = [(i - distance, i) for i in devices if i - distance in devices]
    return lax.ppermute(block, axis, route)


def cut_along(value, dim, count):
    shape = value.shape
    tiles = value.reshape(*shape[:dim], count, shape[dim] // count, *shape[dim + 1 :])
    return jnp.moveaxis(tiles, dim, 0)


def sum_at_owner(value, axis, dim):
    tiles = cut_along(value, dim, lax.axis_size(axis))
    arrived = lax.all_to_all(tiles, axis, split_axis=0, concat_axis=0, tiled=True)
    return arrived.astype(jnp.float32).sum(axis=0)


def attention_kernel(
    ring,
    q_ref,
    kv_ref,
    gate_ref,
    out_ref,
    own,
    other,
    row_max,
    row_sum,
    total,
    s1,
    sr,
    sl,
    sd,
    r_own,
    r_other,
):
    half = ring // 2
    sp = lax.axis_index("sp")
    core = lax.axis_index("tp")
    z, y = sp // ring, sp % ring
    far = 1 - core

    def first_axis(step):
        y1 = (y + far * step + ring) % ring
        z1 = (z + core * step + ring) % ring
        return {"sp": z1 * ring + y1}

    def second_axis(step):
        y1 = (y + core * step + ring) % ring
        z1 = (z + far * step + ring) % ring
        return {"sp": z1 * ring + y1}

    partner = {"tp": far}
    barrier = pltpu.get_barrier_semaphore()
    for who in (first_axis(1), first_axis(-1), second_axis(1), second_axis(-1), partner):
        pl.semaphore_signal(barrier, inc=1, device_id=who, device_id_type=MESH)
    own[0, 0] = kv_ref[...]
    row_max[...] = jnp.full_like(row_max, masked_score)
    row_sum[...] = jnp.zeros_like(row_sum)
    total[...] = jnp.zeros_like(total)
    pl.semaphore_wait(barrier, 5)

    def copy(src, dst, send, recv, who):
        return pltpu.make_async_remote_copy(
            src_ref=src, dst_ref=dst, send_sem=send, recv_sem=recv, device_id=who, device_id_type=MESH
        )

    def along(src, j, step):
        return copy(src, own.at[0, j], s1.at[j], r_own.at[0, j], first_axis(step))

    def right(src, slot, j):
        return copy(src, own.at[slot, j], sr.at[slot, j], r_own.at[slot, j], second_axis(1))

    def left(src, slot, j):
        return copy(src, own.at[slot, j], sl.at[slot, j], r_own.at[slot, j], second_axis(-1))

    def across(src, slot, j):
        return copy(src, other.at[slot, j], sd.at[slot, j], r_other.at[slot, j], partner)

    def arrived(slot, j):
        copy(own.at[slot, j], own.at[slot, j], sd.at[slot, j], r_own.at[slot, j], partner).wait_recv()

    def arrived_other(slot, j):
        copy(other.at[slot, j], other.at[slot, j], sd.at[slot, j], r_other.at[slot, j], partner).wait_recv()

    heads = 2
    rows = q_ref.shape[0] // heads
    depth = q_ref.shape[1]
    block = own.shape[3]
    group = ring // 2
    factor = depth ** (-0.5) * math.log2(math.e)

    def place(slot, j, origin):
        dp = slot - (slot // (half + 1)) * (2 * slot - half)
        ds = (j + 1) // 2 * (2 * (j % 2) - 1)
        z1 = (z - dp + origin * (dp - ds) + 2 * ring) % ring
        y1 = (y - ds + origin * (ds - dp) + 2 * ring) % ring
        return z1 * ring + y1

    def attend(buffer, slot, part, origin, diagonal=False):
        start = part * group
        keys = buffer[slot, pl.ds(start, group), 0].reshape(group * block, depth)
        values = buffer[slot, pl.ds(start, group), 1].reshape(group * block, depth)
        for head in range(heads):
            here = pl.ds(head * rows, rows)
            biases = []
            for i in range(group):
                from_sp = place(slot, start + i, origin)
                bias = jnp.where(from_sp <= sp, 0.0, masked_score).astype(jnp.float32)
                biases.append(gate_ref[head, pl.ds(from_sp * 2 + origin, 1), :] + bias)
            score = lax.dot_general(
                q_ref[here, :], keys, (((1,), (1,)), ((), ())), preferred_element_type=jnp.float32
            )
            score = score * factor + jnp.concatenate(biases, axis=1)
            if diagonal:
                at = lax.broadcasted_iota(jnp.int32, score.shape, 0)
                key = lax.broadcasted_iota(jnp.int32, score.shape, 1)
                hidden = (key < block) & (key + origin * block > at)
                score = jnp.where(hidden, masked_score, score)
            old = row_max[here, :]
            new = jnp.maximum(old, jnp.max(score, axis=1, keepdims=True))
            rescale = jnp.exp2(old - new)
            weight = jnp.exp2(score - jnp.concatenate([new] * (score.shape[1] // 128), axis=1))
            lanes = weight[:, :128]
            for i in range(1, score.shape[1] // 128):
                lanes = lanes + weight[:, i * 128 : (i + 1) * 128]
            row_max[here, :] = new
            row_sum[here, :] = row_sum[here, :] * rescale + lanes
            total[here, :] = total[here, :] * rescale + jnp.dot(
                weight.astype(jnp.bfloat16), values, preferred_element_type=jnp.float32
            )

    for j in range(ring):
        if j == 0:
            piece = kv_ref
            along(piece, 1, 1).start()
            along(piece, 2, -1).start()
        else:
            piece = own.at[0, j]
            arrived(0, j)
            if j + 2 < ring:
                along(piece, j + 2, 1 if j % 2 else -1).start()
        right(piece, 1, j).start()
        left(piece, half + 1, j).start()
        across(piece, 0, j).start()

    for hop in range(1, half):
        r, l = hop, half + hop

        def pass_on(j, odd):
            arrived(r, j)
            if hop < half - 1:
                right(own.at[r, j], r + 1, j).start()
            elif odd:
                right(own.at[r, j], half, j).start()
            across(own.at[r, j], r, j).start()
            arrived(l, j)
            if hop < half - 1:
                left(own.at[l, j], l + 1, j).start()
            elif not odd:
                left(own.at[l, j], half, j).start()
            across(own.at[l, j], l, j).start()

        if hop == 1:

            def wait_other(slot, part):
                for i in range(group):
                    arrived_other(slot, part * group + i)

            for quarter in range(4):
                for i in range(ring // 4):
                    j = quarter * (ring // 4) + i
                    pass_on(j, j % 2)
                if quarter < 2:
                    attend(own, 0, quarter, core, diagonal=quarter == 0)
                else:
                    wait_other(0, quarter - 2)
                    attend(other, 0, quarter - 2, far, diagonal=quarter == 2)
        else:

            def step(t, carry):
                slot = r - 1 + (t // 2) * half
                part = t % 2
                for i in range(ring // 8):
                    pass_on(2 * t, 0)
                attend(own, slot, part, core)
                for i in range(ring // 8):
                    pass_on(2 * t + 1, 1)
                for i in range(group):
                    arrived_other(slot, part * group + i)
                attend(other, slot, part, far)
                return carry

            lax.fori_loop(0, 4, step, 0)

    def last(t, carry):
        slot = half - 1 + (t // 2) * half
        part = t % 2
        for i in range(2):
            arrived(half, 2 * t + i)
            across(own.at[half, 2 * t + i], half, 2 * t + i).start()
        attend(own, slot, part, core)
        for i in range(group):
            arrived_other(slot, part * group + i)
        attend(other, slot, part, far)
        return carry

    lax.fori_loop(0, 4, last, 0)

    def tail(t, carry):
        attend(own, half, t, core)
        for i in range(group):
            arrived_other(half, t * group + i)
        attend(other, half, t, far)
        return carry

    lax.fori_loop(0, 2, tail, 0)

    for head in range(heads):
        here = pl.ds(head * rows, rows)
        out_ref[:, pl.ds(head * depth, depth)] = (
            total[here, :] / jnp.sum(row_sum[here, :], axis=1, keepdims=True)
        ).astype(out_ref.dtype)

    for j in range(1, ring):
        along(own.at[0, j], j, 1).wait_send()

    def sent(j, carry):
        for slot in range(1, half):
            right(own.at[slot, j], slot, j).wait_send()
            left(own.at[half + slot, j], half + slot, j).wait_send()
        for slot in range(ring):
            across(own.at[slot, j], slot, j).wait_send()
        return carry

    lax.fori_loop(0, ring, sent, 0)

    def sent_far(t, carry):
        right(own.at[half, 2 * t + 1], half, 2 * t + 1).wait_send()
        left(own.at[half, 2 * t], half, 2 * t).wait_send()
        return carry

    lax.fori_loop(0, half, sent_far, 0)


def attention(q, kv, gates, ring):
    rows, depth = q.shape
    block = kv.shape[1]
    slots = pltpu.VMEM((ring, ring, 2, block, depth), kv.dtype)
    dma = pltpu.SemaphoreType.DMA
    return pl.pallas_call(
        functools.partial(attention_kernel, ring),
        out_shape=jax.ShapeDtypeStruct((rows // 2, 2 * depth), jnp.bfloat16),
        in_specs=[pl.BlockSpec(memory_space=pltpu.VMEM)] * 3,
        out_specs=pl.BlockSpec(memory_space=pltpu.VMEM),
        scratch_shapes=[
            slots,
            slots,
            pltpu.VMEM((rows, 128), jnp.float32),
            pltpu.VMEM((rows, 128), jnp.float32),
            pltpu.VMEM((rows, depth), jnp.float32),
            dma((ring,)),
            dma((ring, ring)),
            dma((ring, ring)),
            dma((ring, ring)),
            dma((ring, ring)),
            dma((ring, ring)),
        ],
        compiler_params=pltpu.CompilerParams(
            collective_id=0, has_side_effects=True, vmem_limit_bytes=48 << 20
        ),
        cost_estimate=pl.CostEstimate(
            flops=4 * rows * depth * block * 2 * ring * ring, bytes_accessed=1 << 22, transcendentals=0
        ),
        name="gather_attend",
    )(q, kv, gates)


def shards(
    tokens,
    norm_gain,
    w_query,
    w_key,
    w_value,
    w_conv_value,
    w_conv_pre,
    w_conv_post,
    conv_taps,
    log_gate_cache,
    w_out_conv,
    w_out_attn,
):
    float_rows = tokens.astype(jnp.float32)
    scaled = float_rows * lax.rsqrt(
        jnp.mean(float_rows * float_rows, axis=1, keepdims=True) + epsilon
    )
    normed_own = (scaled * norm_gain).astype(jnp.bfloat16)
    normed = gather_directly(normed_own, ("fs", "tp"), 0)
    block_rows = normed.shape[0]
    channels = w_conv_post.shape[1]
    head_dim = w_key.shape[1]
    local_heads = w_query.shape[1] // head_dim
    group = lax.axis_index(("fs", "tp"))
    core_index = lax.axis_index("tp")
    half_rows = block_rows // 2
    own_rows = lax.dynamic_slice_in_dim(normed, core_index * half_rows, half_rows, 0)
    kv = jnp.stack(
        [
            jnp.dot(own_rows, w, preferred_element_type=jnp.float32).astype(jnp.bfloat16)
            for w in (w_key, w_value)
        ]
    )
    queries = jnp.dot(normed, w_query, preferred_element_type=jnp.float32).astype(jnp.bfloat16)
    queries = jnp.moveaxis(queries.reshape(block_rows, local_heads, head_dim), 1, 0)
    head_gates = lax.dynamic_slice_in_dim(log_gate_cache, group * local_heads, local_heads, 0)
    gates = (head_gates * (-math.log2(math.e))).reshape(local_heads, -1, half_rows)
    ring = math.isqrt(lax.axis_size("sp"))
    attn_out = attention(queries.reshape(local_heads * block_rows, head_dim), kv, gates, ring)

    local_weight = jnp.concatenate([w_conv_post, w_conv_pre, w_conv_value], axis=1)
    projected = jnp.dot(normed, local_weight, preferred_element_type=jnp.float32).astype(
        jnp.bfloat16
    )
    post_gate = projected[:, :channels]
    pre_gate = projected[:, channels : 2 * channels]
    conv_value = projected[:, 2 * channels : 3 * channels]
    mixed_in = (pre_gate.astype(jnp.float32) * conv_value.astype(jnp.float32)).astype(jnp.bfloat16)
    kernel = conv_taps.shape[0]
    carried = passed_along(mixed_in[block_rows - (kernel - 1) :], "sp", 1)
    extended = jnp.concatenate([carried, mixed_in], axis=0).astype(jnp.float32)
    tap_weights = lax.dynamic_slice_in_dim(conv_taps, group * channels, channels, 1).astype(
        jnp.float32
    )
    conv_sum = tap_weights[0] * extended[0:block_rows]
    for offset in range(1, kernel):
        conv_sum = conv_sum + tap_weights[offset] * extended[offset : offset + block_rows]
    conv_out = (post_gate.astype(jnp.float32) * conv_sum).astype(jnp.bfloat16)

    mixed = sum_at_owner(
        (
            jnp.dot(conv_out, w_out_conv, preferred_element_type=jnp.float32)
            + jnp.dot(attn_out, w_out_attn, preferred_element_type=jnp.float32)
        ).astype(jnp.bfloat16),
        ("fs", "tp"),
        0,
    )
    return mixed.astype(jnp.bfloat16)


def solution(mesh):
    placed = (
        P(("sp", "fs", "tp"), None),
        P(),
        P(None, ("fs", "tp")),
        P(None, "fs"),
        P(None, "fs"),
        P(None, ("fs", "tp")),
        P(None, ("fs", "tp")),
        P(None, ("fs", "tp")),
        P(),
        P(),
        P(("fs", "tp"), None),
        P(("fs", "tp"), None),
    )
    return jax.shard_map(
        shards, mesh=mesh, in_specs=placed, out_specs=P(("sp", "fs", "tp"), None), check_vma=False
    )
```

```python
import functools
import math

import jax
import jax.numpy as jnp
from jax import lax
from jax.experimental import pallas as pl
from jax.experimental.pallas import tpu as pltpu
from jax.sharding import PartitionSpec as P

epsilon = 1e-06
masked_score = -1e30
MESH = pl.DeviceIdType.MESH
log2_e = math.log2(math.e)


def arrival_order(ring):
    half = ring // 2
    pieces = []
    for slot in range(ring):
        hops = slot if slot <= half else slot - half
        for j in range(ring):
            pieces.append((hops + (j + 1) // 2, hops, slot, j))
    return [(slot, j) for _, _, slot, j in sorted(pieces)]


def chosen(values, t):
    if isinstance(t, int):
        return values[t]
    words = [values[n : n + 8] for n in range(0, len(values), 8)]
    packed = [sum(v << (3 * n) for n, v in enumerate(word)) for word in words]
    picked = jnp.int32(packed[-1])
    for n in range(len(packed) - 2, -1, -1):
        picked = jnp.where(t < 8 * (n + 1), jnp.int32(packed[n]), picked)
    return (picked >> (3 * (t % 8))) & 7


def layer_kernel(
    ring,
    tokens,
    gain,
    w_query,
    w_key,
    w_value,
    w_conv_value,
    w_conv_pre,
    w_conv_post,
    taps,
    log_gates,
    w_out_conv,
    w_out_attn,
    out_ref,
    rows,
    wq,
    wkv,
    wconv,
    wout,
    gates,
    bias_of,
    q_ref,
    own,
    other,
    row_max,
    row_sum,
    total,
    mixed_tail,
    halo,
    extended,
    gate_after,
    merged,
    part_keep,
    part_send,
    part_come,
    pair,
    relay,
    passed,
    come,
    weight_sem,
    gx_send,
    gx_recv,
    gd_send,
    gd_recv,
    halo_sem,
    s1,
    sr,
    sl,
    sd,
    r_own,
    r_other,
    pd_send,
    pd_recv,
    relay_send,
    relay_recv,
    come_send,
    come_recv,
):
    half = ring // 2
    group = ring // 2
    sp = lax.axis_index("sp")
    x = lax.axis_index("fs")
    core = lax.axis_index("tp")
    z, y = sp // ring, sp % ring
    far = 1 - core
    device = x * 2 + core
    blocks = ring * ring
    bf16 = jnp.bfloat16
    f32 = jnp.float32

    def first_axis(step):
        y1 = (y + far * step + ring) % ring
        z1 = (z + core * step + ring) % ring
        return {"sp": z1 * ring + y1}

    def second_axis(step):
        y1 = (y + core * step + ring) % ring
        z1 = (z + far * step + ring) % ring
        return {"sp": z1 * ring + y1}

    def along_x(step):
        return {"fs": (x + step + 4) % 4}

    partner = {"tp": far}
    after = {"sp": (sp + 1) % blocks}
    before = {"sp": (sp + blocks - 1) % blocks}

    def copy(src, dst, send, recv, who):
        return pltpu.make_async_remote_copy(
            src_ref=src, dst_ref=dst, send_sem=send, recv_sem=recv, device_id=who, device_id_type=MESH
        )

    depth = w_key.shape[1]
    channels = w_conv_post.shape[1]
    loads = [
        (log_gates, gates),
        (w_key, wkv.at[:, pl.ds(0, depth)]),
        (w_value, wkv.at[:, pl.ds(depth, depth)]),
        (w_query, wq),
        (w_conv_post, wconv.at[:, pl.ds(0, channels)]),
        (w_conv_pre, wconv.at[:, pl.ds(channels, channels)]),
        (w_conv_value, wconv.at[:, pl.ds(2 * channels, channels)]),
        (w_out_conv, wout.at[pl.ds(0, channels)]),
        (w_out_attn, wout.at[pl.ds(channels, 2 * depth)]),
    ]
    loads = [pltpu.make_async_copy(a, b, weight_sem.at[n]) for n, (a, b) in enumerate(loads)]
    for load in loads:
        load.start()

    barrier = pltpu.get_barrier_semaphore()
    near = (
        first_axis(1),
        first_axis(-1),
        second_axis(1),
        second_axis(-1),
        partner,
        along_x(1),
        along_x(-1),
        after,
        before,
    )
    for who in near:
        pl.semaphore_signal(barrier, inc=1, device_id=who, device_id_type=MESH)

    wide = tokens[...].astype(f32)
    scaled = wide * lax.rsqrt(jnp.mean(wide * wide, axis=1, keepdims=True) + epsilon)
    rows[device] = (scaled * gain[...]).astype(bf16)
    row_max[...] = jnp.full_like(row_max, masked_score)
    row_sum[...] = jnp.zeros_like(row_sum)
    total[...] = jnp.zeros_like(total)
    pl.semaphore_wait(barrier, len(near))

    few = rows.shape[1] // 2

    def of_x(step):
        return (x + step + 4) % 4 * 2 + core

    def piece_of(step, h):
        return rows.at[of_x(step), pl.ds(h * few, few)]

    def gather_x(step, h, sem, way):
        return copy(piece_of(step, h), piece_of(step, h), gx_send.at[sem], gx_recv.at[sem], along_x(way))

    def gather_across(step, n):
        here = rows.at[of_x(step)]
        return copy(here, here, gd_send.at[n], gd_recv.at[n], partner)

    def came_x(step, h, sem):
        return copy(piece_of(step, h), piece_of(step, h), gx_send.at[sem], gx_recv.at[sem], partner)

    first = [
        gather_x(0, 0, 0, 1),
        gather_x(0, 1, 1, -1),
        gather_x(0, 1, 2, 1),
        gather_x(0, 0, 3, -1),
    ]
    for one in first:
        one.start()
    crossing = [gather_across(0, 0)]
    crossing[0].start()

    heads = 2
    keys_of_block = bias_of.shape[2]
    loads[0].wait()
    row = lax.broadcasted_iota(jnp.int32, (gates.shape[0], keys_of_block), 0)
    for head in range(heads):
        mine = row == device * heads + head
        for n in range(0, bias_of.shape[1], 8):
            lines = [
                jnp.sum(
                    jnp.where(mine, gates[:, b * keys_of_block : (b + 1) * keys_of_block], 0.0),
                    axis=0,
                    keepdims=True,
                )
                for b in range(n, n + 8)
            ]
            seen = n + lax.broadcasted_iota(jnp.int32, (8, keys_of_block), 0) < 2 * sp + 2
            bias_of[head, n : n + 8] = jnp.where(
                seen, jnp.concatenate(lines, axis=0) * -log2_e, masked_score
            )

    came_x(-1, 0, 0).wait_recv()
    second = [gather_x(-1, 0, 4, 1)]
    second[0].start()
    came_x(1, 1, 1).wait_recv()
    second.append(gather_x(1, 1, 5, -1))
    second[1].start()
    came_x(-1, 1, 2).wait_recv()
    crossing.append(gather_across(-1, 1))
    crossing[1].start()
    came_x(1, 0, 3).wait_recv()
    crossing.append(gather_across(1, 2))
    crossing[2].start()
    came_x(2, 0, 4).wait_recv()
    came_x(2, 1, 5).wait_recv()
    crossing.append(gather_across(2, 3))
    crossing[3].start()
    for n in range(4):
        here = rows.at[(x + (0, -1, 1, 2)[n] + 4) % 4 * 2 + far]
        copy(here, here, gd_send.at[n], gd_recv.at[n], partner).wait_recv()

    width = rows.shape[2]
    block = own.shape[3]
    loads[1].wait()
    loads[2].wait()
    half_rows = rows[pl.ds(4 * core, 4)].reshape(block, width)
    made = jnp.dot(half_rows, wkv[...], preferred_element_type=f32).astype(bf16)
    own[0, 0, 0] = made[:, :depth]
    own[0, 0, 1] = made[:, depth:]

    def along(src, j, step):
        return copy(src, own.at[0, j], s1.at[j], r_own.at[0, j], first_axis(step))

    def right(src, slot, j):
        return copy(src, own.at[slot, j], sr.at[slot, j], r_own.at[slot, j], second_axis(1))

    def left(src, slot, j):
        return copy(src, own.at[slot, j], sl.at[slot, j], r_own.at[slot, j], second_axis(-1))

    def across(src, slot, j):
        return copy(src, other.at[slot, j], sd.at[slot, j], r_other.at[slot, j], partner)

    def arrived(slot, j):
        copy(own.at[slot, j], own.at[slot, j], sd.at[slot, j], r_own.at[slot, j], partner).wait_recv()

    def arrived_other(slot, j):
        copy(other.at[slot, j], other.at[slot, j], sd.at[slot, j], r_other.at[slot, j], partner).wait_recv()

    here = own.at[0, 0]
    along(here, 1, 1).start()
    along(here, 2, -1).start()
    right(here, 1, 0).start()
    left(here, half + 1, 0).start()
    across(here, 0, 0).start()

    span = rows.shape[0] * rows.shape[1]
    all_rows = rows[...].reshape(span, width)
    loads[3].wait()
    asked = jnp.dot(all_rows, wq[...], preferred_element_type=f32).astype(bf16)
    for head in range(heads):
        q_ref[pl.ds(head * span, span), :] = asked[:, head * depth : (head + 1) * depth]
    for n in (4, 5, 6):
        loads[n].wait()
    projected = jnp.dot(all_rows, wconv[...], preferred_element_type=f32).astype(bf16)
    gate_after[...] = projected[:, :channels]
    mixed_in = (
        projected[:, channels : 2 * channels].astype(f32) * projected[:, 2 * channels :].astype(f32)
    ).astype(bf16)
    edge = halo.shape[0]
    mixed_tail[...] = mixed_in[span - edge :]
    extended[pl.ds(edge, span), :] = mixed_in.astype(f32)
    shift = copy(mixed_tail, halo, halo_sem.at[0], halo_sem.at[1], after)
    shift.start()
    factor = depth ** (-0.5) * log2_e

    def place(slot, j, origin):
        dp = slot - (slot // (half + 1)) * (2 * slot - half)
        ds = (j + 1) // 2 * (2 * (j % 2) - 1)
        z1 = (z - dp + origin * (dp - ds) + 2 * ring) % ring
        y1 = (y - ds + origin * (ds - dp) + 2 * ring) % ring
        return z1 * ring + y1

    def attend(buffer, pieces, origin, diagonal=False):
        keys = jnp.concatenate([buffer[slot, j, 0] for slot, j in pieces], axis=0)
        values = jnp.concatenate([buffer[slot, j, 1] for slot, j in pieces], axis=0)
        for head in range(heads):
            here = pl.ds(head * span, span)
            biases = []
            for slot, j in pieces:
                biases.append(bias_of[head, pl.ds(place(slot, j, origin) * 2 + origin, 1), :])
            score = lax.dot_general(
                q_ref[here, :], keys, (((1,), (1,)), ((), ())), preferred_element_type=f32
            )
            score = score * factor + jnp.concatenate(biases, axis=1)
            if diagonal:
                at = lax.broadcasted_iota(jnp.int32, score.shape, 0)
                key = lax.broadcasted_iota(jnp.int32, score.shape, 1)
                hidden = (key < block) & (key + origin * block > at)
                score = jnp.where(hidden, masked_score, score)
            old = row_max[here, :]
            new = jnp.maximum(old, jnp.max(score, axis=1, keepdims=True))
            rescale = jnp.exp2(old - new)
            weight = jnp.exp2(score - jnp.concatenate([new] * (score.shape[1] // 128), axis=1))
            lanes = weight[:, :128]
            for i in range(1, score.shape[1] // 128):
                lanes = lanes + weight[:, i * 128 : (i + 1) * 128]
            row_max[here, :] = new
            row_sum[here, :] = row_sum[here, :] * rescale + lanes
            total[here, :] = total[here, :] * rescale + jnp.dot(
                weight.astype(bf16), values, preferred_element_type=f32
            )

    order = arrival_order(ring)
    turns = len(order) // group

    def at_turn(t, i):
        slots = [order[n * group + i][0] for n in range(turns)]
        places = [order[n * group + i][1] for n in range(turns)]
        return chosen(slots, t), chosen(places, t)

    def pass_on(t):
        for i in range(group):
            slot, j = at_turn(t, i)
            here = own.at[slot, j]
            arrived(slot, j)
            odd = j % 2

            @pl.when((slot == 0) & (j + 2 < ring))
            def _():
                along(here, j + 2, 2 * odd - 1).start()

            @pl.when((slot < half - 1) | ((slot == half - 1) & (odd == 1)))
            def _():
                right(here, slot + 1, j).start()

            down = jnp.where(slot == 0, half, slot)

            @pl.when((slot == 0) | ((slot > half) & ((slot < ring - 1) | (odd == 0))))
            def _():
                left(here, jnp.where(slot == ring - 1, half, down + 1), j).start()

            across(here, slot, j).start()

    def attend_turn(t, diagonal=False):
        pieces = [at_turn(t, i) for i in range(group)]
        attend(own, pieces, core, diagonal)
        for slot, j in pieces:
            arrived_other(slot, j)
        attend(other, pieces, far, diagonal)

    for i in range(1, group):
        slot, j = order[i]
        here = own.at[slot, j]
        arrived(slot, j)
        if slot == 0:
            along(here, j + 2, 2 * (j % 2) - 1).start()
            left(here, half + 1, j).start()
        if slot > half:
            left(here, slot + 1, j).start()
        else:
            right(here, slot + 1, j).start()
        across(here, slot, j).start()
    pass_on(jnp.int32(1))
    attend_turn(0, diagonal=True)

    def turn(t, carry):
        pass_on(t)
        attend_turn(t - 1)
        return carry

    lax.fori_loop(2, turns, turn, 0)

    shift.wait()
    extended[pl.ds(0, edge), :] = jnp.where(sp == 0, 0.0, halo[...].astype(f32))
    at = pl.multiple_of(device * channels, channels)
    tap_rows = taps[:, pl.ds(at, channels)].astype(f32)
    count = tap_rows.shape[0]
    conv_sum = tap_rows[0:1] * extended[pl.ds(edge - count + 1, span), :]
    for n in range(1, count):
        conv_sum = conv_sum + tap_rows[n : n + 1] * extended[pl.ds(edge - count + 1 + n, span), :]
    merged[:, pl.ds(0, channels)] = (gate_after[...].astype(f32) * conv_sum).astype(bf16)

    attend_turn(turns - 1)
    for head in range(heads):
        here = pl.ds(head * span, span)
        merged[:, pl.ds(channels + head * depth, depth)] = (
            total[here, :] / jnp.sum(row_sum[here, :], axis=1, keepdims=True)
        ).astype(bf16)

    loads[7].wait()
    loads[8].wait()
    chunks = part_keep.shape[0]
    columns = part_keep.shape[3]

    def to_partner(k):
        return copy(part_send.at[k], part_come.at[k], pd_send.at[k], pd_recv.at[k], partner)

    def way(k):
        return 1 if k % 2 == 0 else -1

    def to_relay(k):
        return copy(pair.at[k, (x + 2) % 4], relay.at[k], relay_send.at[k], relay_recv.at[k], along_x(way(k)))

    def straight(k):
        return copy(
            pair.at[k, (x - way(k) + 4) % 4],
            come.at[k, 1],
            come_send.at[k, 1],
            come_recv.at[k, 1],
            along_x(-way(k)),
        )

    def relayed(k):
        return copy(passed.at[k], come.at[k, 0], come_send.at[k, 0], come_recv.at[k, 0], along_x(way(k)))

    def project(k):
        part = jnp.dot(
            merged[...], wout[:, pl.ds(k * columns, columns)], preferred_element_type=f32
        ).astype(bf16)
        part = part.reshape(4, 2, span // 8, columns)
        part_send[k] = jnp.where(core == 0, part[:, 1], part[:, 0])
        part_keep[k] = jnp.where(core == 0, part[:, 0], part[:, 1])
        to_partner(k).start()

    def add_pair(k):
        to_partner(k).wait_recv()
        pair[k] = (part_keep[k].astype(f32) + part_come[k].astype(f32)).astype(bf16)
        to_relay(k).start()
        straight(k).start()

    def add_relay(k):
        to_relay(k).wait_recv()
        mine = pair[k, (x + way(k) + 4) % 4].astype(f32)
        passed[k] = (mine + relay[k].astype(f32)).astype(bf16)
        relayed(k).start()

    def finish(k):
        straight(k).wait_recv()
        relayed(k).wait_recv()
        out_ref[:, pl.ds(k * columns, columns)] = (
            pair[k, x].astype(f32) + come[k, 0].astype(f32) + come[k, 1].astype(f32)
        ).astype(out_ref.dtype)

    for k in range(chunks + 2):
        if k < chunks:
            project(k)
        if 0 < k < chunks + 1:
            add_pair(k - 1)
        if k > 1:
            add_relay(k - 2)
    for k in range(chunks):
        finish(k)

    for one in first + second + crossing:
        one.wait_send()
    for k in range(chunks):
        to_partner(k).wait_send()
        to_relay(k).wait_send()
        straight(k).wait_send()
        relayed(k).wait_send()
    for j in range(1, ring):
        along(own.at[0, j], j, 1).wait_send()

    def sent(j, carry):
        for slot in range(1, half):
            right(own.at[slot, j], slot, j).wait_send()
            left(own.at[half + slot, j], half + slot, j).wait_send()
        for slot in range(ring):
            across(own.at[slot, j], slot, j).wait_send()
        return carry

    lax.fori_loop(0, ring, sent, 0)

    def sent_far(t, carry):
        right(own.at[half, 2 * t + 1], half, 2 * t + 1).wait_send()
        left(own.at[half, 2 * t], half, 2 * t).wait_send()
        return carry

    lax.fori_loop(0, half, sent_far, 0)


def shards(
    tokens,
    norm_gain,
    w_query,
    w_key,
    w_value,
    w_conv_value,
    w_conv_pre,
    w_conv_post,
    conv_taps,
    log_gate_cache,
    w_out_conv,
    w_out_attn,
):
    ring = math.isqrt(lax.axis_size("sp"))
    few, width = tokens.shape
    span = 8 * few
    depth = w_key.shape[1]
    channels = w_conv_post.shape[1]
    heads = w_query.shape[1] // depth
    block = span // 2
    chunks = 4
    columns = width // chunks
    bf16, f32 = jnp.bfloat16, jnp.float32
    dma = pltpu.SemaphoreType.DMA
    vmem = pltpu.VMEM
    here = pl.BlockSpec(memory_space=pltpu.VMEM)
    away = pl.BlockSpec(memory_space=pl.ANY)
    slots = vmem((ring, ring, 2, block, depth), bf16)
    return pl.pallas_call(
        functools.partial(layer_kernel, ring),
        out_shape=jax.ShapeDtypeStruct((few, width), bf16),
        in_specs=[here, here] + [away] * 6 + [here] + [away] * 3,
        out_specs=here,
        scratch_shapes=[
            vmem((8, few, width), bf16),
            vmem((width, heads * depth), bf16),
            vmem((width, 2 * depth), bf16),
            vmem((width, 3 * channels), bf16),
            vmem((channels + heads * depth, width), bf16),
            vmem(log_gate_cache.shape, f32),
            vmem((heads, 2 * ring * ring, block), f32),
            vmem((heads * span, depth), bf16),
            slots,
            slots,
            vmem((heads * span, 128), f32),
            vmem((heads * span, 128), f32),
            vmem((heads * span, depth), f32),
            vmem((16, channels), bf16),
            vmem((16, channels), bf16),
            vmem((span + 16, channels), f32),
            vmem((span, channels), bf16),
            vmem((span, channels + heads * depth), bf16),
            vmem((chunks, 4, few, columns), bf16),
            vmem((chunks, 4, few, columns), bf16),
            vmem((chunks, 4, few, columns), bf16),
            vmem((chunks, 4, few, columns), bf16),
            vmem((chunks, few, columns), bf16),
            vmem((chunks, few, columns), bf16),
            vmem((chunks, 2, few, columns), bf16),
            dma((9,)),
            dma((6,)),
            dma((6,)),
            dma((4,)),
            dma((4,)),
            dma((2,)),
            dma((ring,)),
            dma((ring, ring)),
            dma((ring, ring)),
            dma((ring, ring)),
            dma((ring, ring)),
            dma((ring, ring)),
            dma((chunks,)),
            dma((chunks,)),
            dma((chunks,)),
            dma((chunks,)),
            dma((chunks, 2)),
            dma((chunks, 2)),
        ],
        compiler_params=pltpu.CompilerParams(
            collective_id=0, has_side_effects=True, vmem_limit_bytes=60 << 20
        ),
        name="layer",
    )(
        tokens,
        norm_gain.reshape(1, width),
        w_query,
        w_key,
        w_value,
        w_conv_value,
        w_conv_pre,
        w_conv_post,
        conv_taps,
        log_gate_cache,
        w_out_conv,
        w_out_attn,
    )


def solution(mesh):
    placed = (
        P(("sp", "fs", "tp"), None),
        P(),
        P(None, ("fs", "tp")),
        P(None, "fs"),
        P(None, "fs"),
        P(None, ("fs", "tp")),
        P(None, ("fs", "tp")),
        P(None, ("fs", "tp")),
        P(),
        P(),
        P(("fs", "tp"), None),
        P(("fs", "tp"), None),
    )
    return jax.shard_map(
        shards, mesh=mesh, in_specs=placed, out_specs=P(("sp", "fs", "tp"), None), check_vma=False
    )
```

```python
import functools
import math

import jax
import jax.numpy as jnp
from jax import lax
from jax.experimental import pallas as pl
from jax.experimental.pallas import tpu as pltpu
from jax.sharding import PartitionSpec as P

epsilon = 1e-06
masked_score = -1e30
MESH = pl.DeviceIdType.MESH
log2_e = math.log2(math.e)


def arrival_order(ring):
    half = ring // 2
    pieces = []
    for slot in range(ring):
        hops = slot if slot <= half else slot - half
        for j in range(ring):
            pieces.append((hops + (j + 1) // 2, hops, slot, j))
    return [(slot, j) for _, _, slot, j in sorted(pieces)]


def chosen(values, t):
    if isinstance(t, int):
        return values[t]
    words = [values[n : n + 8] for n in range(0, len(values), 8)]
    packed = [sum(v << (3 * n) for n, v in enumerate(word)) for word in words]
    picked = jnp.int32(packed[-1])
    for n in range(len(packed) - 2, -1, -1):
        picked = jnp.where(t < 8 * (n + 1), jnp.int32(packed[n]), picked)
    return (picked >> (3 * (t % 8))) & 7


def layer_kernel(
    ring,
    tokens,
    gain,
    w_query,
    w_key,
    w_value,
    w_conv_value,
    w_conv_pre,
    w_conv_post,
    taps,
    log_gates,
    w_out_conv,
    w_out_attn,
    out_ref,
    rows,
    wq,
    wkv,
    wconv,
    wout,
    gates,
    bias_of,
    q_ref,
    own,
    other,
    row_max,
    row_sum,
    total,
    mixed_tail,
    halo,
    extended,
    gate_after,
    merged,
    part_keep,
    part_send,
    part_come,
    pair,
    relay,
    passed,
    come,
    weight_sem,
    gx_send,
    gx_recv,
    gd_send,
    gd_recv,
    halo_sem,
    s1,
    sr,
    sl,
    sd,
    r_own,
    r_other,
    pd_send,
    pd_recv,
    relay_send,
    relay_recv,
    come_send,
    come_recv,
):
    half = ring // 2
    group = ring // 2
    sp = lax.axis_index("sp")
    x = lax.axis_index("fs")
    core = lax.axis_index("tp")
    z, y = sp // ring, sp % ring
    far = 1 - core
    device = x * 2 + core
    blocks = ring * ring
    bf16 = jnp.bfloat16
    f32 = jnp.float32

    def first_axis(step):
        y1 = (y + far * step + ring) % ring
        z1 = (z + core * step + ring) % ring
        return {"sp": z1 * ring + y1}

    def second_axis(step):
        y1 = (y + core * step + ring) % ring
        z1 = (z + far * step + ring) % ring
        return {"sp": z1 * ring + y1}

    def along_x(step):
        return {"fs": (x + step + 4) % 4}

    partner = {"tp": far}
    after = {"sp": (sp + 1) % blocks}
    before = {"sp": (sp + blocks - 1) % blocks}

    def copy(src, dst, send, recv, who):
        return pltpu.make_async_remote_copy(
            src_ref=src, dst_ref=dst, send_sem=send, recv_sem=recv, device_id=who, device_id_type=MESH
        )

    depth = w_key.shape[1]
    channels = w_conv_post.shape[1]
    loads = [
        (log_gates, gates),
        (w_key, wkv.at[:, pl.ds(0, depth)]),
        (w_value, wkv.at[:, pl.ds(depth, depth)]),
        (w_query, wq),
        (w_conv_post, wconv.at[:, pl.ds(0, channels)]),
        (w_conv_pre, wconv.at[:, pl.ds(channels, channels)]),
        (w_conv_value, wconv.at[:, pl.ds(2 * channels, channels)]),
        (w_out_conv, wout.at[pl.ds(0, channels)]),
        (w_out_attn, wout.at[pl.ds(channels, 2 * depth)]),
    ]
    loads = [pltpu.make_async_copy(a, b, weight_sem.at[n]) for n, (a, b) in enumerate(loads)]
    for load in loads:
        load.start()

    barrier = pltpu.get_barrier_semaphore()
    near = (
        first_axis(1),
        first_axis(-1),
        second_axis(1),
        second_axis(-1),
        partner,
        along_x(1),
        along_x(-1),
        after,
        before,
    )
    for who in near:
        pl.semaphore_signal(barrier, inc=1, device_id=who, device_id_type=MESH)

    wide = tokens[...].astype(f32)
    scaled = wide * lax.rsqrt(jnp.mean(wide * wide, axis=1, keepdims=True) + epsilon)
    rows[device] = (scaled * gain[...]).astype(bf16)
    row_max[...] = jnp.full_like(row_max, masked_score)
    row_sum[...] = jnp.zeros_like(row_sum)
    total[...] = jnp.zeros_like(total)
    pl.semaphore_wait(barrier, len(near))

    few = rows.shape[1] // 2

    def of_x(step):
        return (x + step + 4) % 4 * 2 + core

    def piece_of(step, h):
        return rows.at[of_x(step), pl.ds(h * few, few)]

    def gather_x(step, h, sem, way):
        return copy(piece_of(step, h), piece_of(step, h), gx_send.at[sem], gx_recv.at[sem], along_x(way))

    def gather_across(step, n):
        here = rows.at[of_x(step)]
        return copy(here, here, gd_send.at[n], gd_recv.at[n], partner)

    def came_x(step, h, sem):
        return copy(piece_of(step, h), piece_of(step, h), gx_send.at[sem], gx_recv.at[sem], partner)

    first = [
        gather_x(0, 0, 0, 1),
        gather_x(0, 1, 1, -1),
        gather_x(0, 1, 2, 1),
        gather_x(0, 0, 3, -1),
    ]
    for one in first:
        one.start()
    crossing = [gather_across(0, 0)]
    crossing[0].start()

    heads = 2
    keys_of_block = bias_of.shape[2]
    loads[0].wait()
    row = lax.broadcasted_iota(jnp.int32, (gates.shape[0], keys_of_block), 0)
    for head in range(heads):
        mine = row == device * heads + head
        for n in range(0, bias_of.shape[1], 8):
            lines = [
                jnp.sum(
                    jnp.where(mine, gates[:, b * keys_of_block : (b + 1) * keys_of_block], 0.0),
                    axis=0,
                    keepdims=True,
                )
                for b in range(n, n + 8)
            ]
            seen = n + lax.broadcasted_iota(jnp.int32, (8, keys_of_block), 0) < 2 * sp + 2
            bias_of[head, n : n + 8] = jnp.where(
                seen, jnp.concatenate(lines, axis=0) * -log2_e, masked_score
            )

    came_x(-1, 0, 0).wait_recv()
    second = [gather_x(-1, 0, 4, 1)]
    second[0].start()
    came_x(1, 1, 1).wait_recv()
    second.append(gather_x(1, 1, 5, -1))
    second[1].start()
    came_x(-1, 1, 2).wait_recv()
    crossing.append(gather_across(-1, 1))
    crossing[1].start()
    came_x(1, 0, 3).wait_recv()
    crossing.append(gather_across(1, 2))
    crossing[2].start()
    came_x(2, 0, 4).wait_recv()
    came_x(2, 1, 5).wait_recv()
    crossing.append(gather_across(2, 3))
    crossing[3].start()
    for n in range(4):
        here = rows.at[(x + (0, -1, 1, 2)[n] + 4) % 4 * 2 + far]
        copy(here, here, gd_send.at[n], gd_recv.at[n], partner).wait_recv()

    width = rows.shape[2]
    block = own.shape[3]
    loads[1].wait()
    loads[2].wait()
    half_rows = rows[pl.ds(4 * core, 4)].reshape(block, width)
    made = jnp.dot(half_rows, wkv[...], preferred_element_type=f32).astype(bf16)
    own[0, 0, 0] = made[:, :depth]
    own[0, 0, 1] = made[:, depth:]

    def along(src, j, step):
        return copy(src, own.at[0, j], s1.at[j], r_own.at[0, j], first_axis(step))

    def right(src, slot, j):
        return copy(src, own.at[slot, j], sr.at[slot, j], r_own.at[slot, j], second_axis(1))

    def left(src, slot, j):
        return copy(src, own.at[slot, j], sl.at[slot, j], r_own.at[slot, j], second_axis(-1))

    def across(src, slot, j):
        return copy(src, other.at[slot, j], sd.at[slot, j], r_other.at[slot, j], partner)

    def arrived(slot, j):
        copy(own.at[slot, j], own.at[slot, j], sd.at[slot, j], r_own.at[slot, j], partner).wait_recv()

    def arrived_other(slot, j):
        copy(other.at[slot, j], other.at[slot, j], sd.at[slot, j], r_other.at[slot, j], partner).wait_recv()

    here = own.at[0, 0]
    along(here, 1, 1).start()
    along(here, 2, -1).start()
    right(here, 1, 0).start()
    left(here, half + 1, 0).start()
    across(here, 0, 0).start()

    span = rows.shape[0] * rows.shape[1]
    all_rows = rows[...].reshape(span, width)
    loads[3].wait()
    asked = jnp.dot(all_rows, wq[...], preferred_element_type=f32).astype(bf16)
    for head in range(heads):
        q_ref[pl.ds(head * span, span), :] = asked[:, head * depth : (head + 1) * depth]
    for n in (4, 5, 6):
        loads[n].wait()
    projected = jnp.dot(all_rows, wconv[...], preferred_element_type=f32).astype(bf16)
    gate_after[...] = projected[:, :channels]
    mixed_in = (
        projected[:, channels : 2 * channels].astype(f32) * projected[:, 2 * channels :].astype(f32)
    ).astype(bf16)
    edge = halo.shape[0]
    mixed_tail[...] = mixed_in[span - edge :]
    extended[pl.ds(edge, span), :] = mixed_in.astype(f32)
    shift = copy(mixed_tail, halo, halo_sem.at[0], halo_sem.at[1], after)
    shift.start()
    factor = depth ** (-0.5) * log2_e

    def place(slot, j, origin):
        dp = slot - (slot // (half + 1)) * (2 * slot - half)
        ds = (j + 1) // 2 * (2 * (j % 2) - 1)
        z1 = (z - dp + origin * (dp - ds) + 2 * ring) % ring
        y1 = (y - ds + origin * (ds - dp) + 2 * ring) % ring
        return z1 * ring + y1

    def attend(parts, pieces, diagonal=False):
        blocks_of = [(buffer, slot, j, origin) for buffer, origin in parts for slot, j in pieces]

        def score_of(unit):
            head, some = unit
            keys = jnp.concatenate([buffer[slot, j, 0] for buffer, slot, j, _ in some], axis=0)
            return lax.dot_general(
                q_ref[pl.ds(head * span, span), :],
                keys,
                (((1,), (1,)), ((), ())),
                preferred_element_type=f32,
            )

        def absorb(score, unit):
            head, some = unit
            here = pl.ds(head * span, span)
            values = jnp.concatenate([buffer[slot, j, 1] for buffer, slot, j, _ in some], axis=0)
            parts_of = []
            for n, (_, slot, j, origin) in enumerate(some):
                bias = bias_of[head, pl.ds(place(slot, j, origin) * 2 + origin, 1), :]
                part = score[:, n * block : (n + 1) * block] * factor + bias
                if diagonal and slot == 0 and j == 0:
                    at = lax.broadcasted_iota(jnp.int32, part.shape, 0)
                    key = lax.broadcasted_iota(jnp.int32, part.shape, 1)
                    part = jnp.where(key + origin * block > at, masked_score, part)
                parts_of.append(part)
            top = parts_of[0]
            for part in parts_of[1:]:
                top = jnp.maximum(top, part)
            old = row_max[here, :]
            new = jnp.maximum(old, jnp.max(top, axis=1, keepdims=True))
            rescale = jnp.exp2(old - new)
            weights = [jnp.exp2(part - new) for part in parts_of]
            lanes = weights[0]
            for weight in weights[1:]:
                lanes = lanes + weight
            row_max[here, :] = new
            row_sum[here, :] = row_sum[here, :] * rescale + lanes
            weight = jnp.concatenate([weight.astype(bf16) for weight in weights], axis=1)
            total[here, :] = total[here, :] * rescale + jnp.dot(
                weight, values, preferred_element_type=f32
            )

        units = [(head, blocks_of) for head in range(heads)]
        ahead = [score_of(unit) for unit in units[:1]]
        for n, unit in enumerate(units):
            if n + 1 < len(units):
                ahead.append(score_of(units[n + 1]))
            absorb(ahead[n], unit)

    order = arrival_order(ring)
    turns = len(order) // group

    def at_turn(t, i):
        slots = [order[n * group + i][0] for n in range(turns)]
        places = [order[n * group + i][1] for n in range(turns)]
        return chosen(slots, t), chosen(places, t)

    def pass_on(t):
        for i in range(group):
            slot, j = at_turn(t, i)
            here = own.at[slot, j]
            arrived(slot, j)
            odd = j % 2

            @pl.when((slot == 0) & (j + 2 < ring))
            def _():
                along(here, j + 2, 2 * odd - 1).start()

            @pl.when((slot < half - 1) | ((slot == half - 1) & (odd == 1)))
            def _():
                right(here, slot + 1, j).start()

            down = jnp.where(slot == 0, half, slot)

            @pl.when((slot == 0) | ((slot > half) & ((slot < ring - 1) | (odd == 0))))
            def _():
                left(here, jnp.where(slot == ring - 1, half, down + 1), j).start()

            across(here, slot, j).start()

    def attend_turn(t, diagonal=False):
        pieces = [at_turn(t, i) for i in range(group)]
        for slot, j in pieces:
            arrived_other(slot, j)
        attend(((own, core), (other, far)), pieces, diagonal)

    for i in range(1, group):
        slot, j = order[i]
        here = own.at[slot, j]
        arrived(slot, j)
        if slot == 0:
            along(here, j + 2, 2 * (j % 2) - 1).start()
            left(here, half + 1, j).start()
        if slot > half:
            left(here, slot + 1, j).start()
        else:
            right(here, slot + 1, j).start()
        across(here, slot, j).start()
    pass_on(jnp.int32(1))
    attend_turn(0, diagonal=True)

    def turn(t, carry):
        pass_on(t)
        attend_turn(t - 1)
        return carry

    lax.fori_loop(2, turns, turn, 0)

    shift.wait()
    extended[pl.ds(0, edge), :] = jnp.where(sp == 0, 0.0, halo[...].astype(f32))
    at = pl.multiple_of(device * channels, channels)
    tap_rows = taps[:, pl.ds(at, channels)].astype(f32)
    count = tap_rows.shape[0]
    conv_sum = tap_rows[0:1] * extended[pl.ds(edge - count + 1, span), :]
    for n in range(1, count):
        conv_sum = conv_sum + tap_rows[n : n + 1] * extended[pl.ds(edge - count + 1 + n, span), :]
    merged[:, pl.ds(0, channels)] = (gate_after[...].astype(f32) * conv_sum).astype(bf16)

    attend_turn(turns - 1)
    for head in range(heads):
        here = pl.ds(head * span, span)
        merged[:, pl.ds(channels + head * depth, depth)] = (
            total[here, :] / jnp.sum(row_sum[here, :], axis=1, keepdims=True)
        ).astype(bf16)

    loads[7].wait()
    loads[8].wait()
    chunks = part_keep.shape[0]
    columns = part_keep.shape[3]

    def to_partner(k):
        return copy(part_send.at[k], part_come.at[k], pd_send.at[k], pd_recv.at[k], partner)

    def way(k):
        return 1 if k % 2 == 0 else -1

    def to_relay(k):
        return copy(pair.at[k, (x + 2) % 4], relay.at[k], relay_send.at[k], relay_recv.at[k], along_x(way(k)))

    def straight(k):
        return copy(
            pair.at[k, (x - way(k) + 4) % 4],
            come.at[k, 1],
            come_send.at[k, 1],
            come_recv.at[k, 1],
            along_x(-way(k)),
        )

    def relayed(k):
        return copy(passed.at[k], come.at[k, 0], come_send.at[k, 0], come_recv.at[k, 0], along_x(way(k)))

    def project(k):
        part = jnp.dot(
            merged[...], wout[:, pl.ds(k * columns, columns)], preferred_element_type=f32
        ).astype(bf16)
        part = part.reshape(4, 2, span // 8, columns)
        part_send[k] = jnp.where(core == 0, part[:, 1], part[:, 0])
        part_keep[k] = jnp.where(core == 0, part[:, 0], part[:, 1])
        to_partner(k).start()

    def add_pair(k):
        to_partner(k).wait_recv()
        pair[k] = (part_keep[k].astype(f32) + part_come[k].astype(f32)).astype(bf16)
        to_relay(k).start()
        straight(k).start()

    def add_relay(k):
        to_relay(k).wait_recv()
        mine = pair[k, (x + way(k) + 4) % 4].astype(f32)
        passed[k] = (mine + relay[k].astype(f32)).astype(bf16)
        relayed(k).start()

    def finish(k):
        straight(k).wait_recv()
        relayed(k).wait_recv()
        out_ref[:, pl.ds(k * columns, columns)] = (
            pair[k, x].astype(f32) + come[k, 0].astype(f32) + come[k, 1].astype(f32)
        ).astype(out_ref.dtype)

    for k in range(chunks + 2):
        if k < chunks:
            project(k)
        if 0 < k < chunks + 1:
            add_pair(k - 1)
        if k > 1:
            add_relay(k - 2)
    for k in range(chunks):
        finish(k)

    for one in first + second + crossing:
        one.wait_send()
    for k in range(chunks):
        to_partner(k).wait_send()
        to_relay(k).wait_send()
        straight(k).wait_send()
        relayed(k).wait_send()
    for j in range(1, ring):
        along(own.at[0, j], j, 1).wait_send()

    def sent(j, carry):
        for slot in range(1, half):
            right(own.at[slot, j], slot, j).wait_send()
            left(own.at[half + slot, j], half + slot, j).wait_send()
        for slot in range(ring):
            across(own.at[slot, j], slot, j).wait_send()
        return carry

    lax.fori_loop(0, ring, sent, 0)

    def sent_far(t, carry):
        right(own.at[half, 2 * t + 1], half, 2 * t + 1).wait_send()
        left(own.at[half, 2 * t], half, 2 * t).wait_send()
        return carry

    lax.fori_loop(0, half, sent_far, 0)


def shards(
    tokens,
    norm_gain,
    w_query,
    w_key,
    w_value,
    w_conv_value,
    w_conv_pre,
    w_conv_post,
    conv_taps,
    log_gate_cache,
    w_out_conv,
    w_out_attn,
):
    ring = math.isqrt(lax.axis_size("sp"))
    few, width = tokens.shape
    span = 8 * few
    depth = w_key.shape[1]
    channels = w_conv_post.shape[1]
    heads = w_query.shape[1] // depth
    block = span // 2
    chunks = 4
    columns = width // chunks
    bf16, f32 = jnp.bfloat16, jnp.float32
    dma = pltpu.SemaphoreType.DMA
    vmem = pltpu.VMEM
    here = pl.BlockSpec(memory_space=pltpu.VMEM)
    away = pl.BlockSpec(memory_space=pl.ANY)
    slots = vmem((ring, ring, 2, block, depth), bf16)
    return pl.pallas_call(
        functools.partial(layer_kernel, ring),
        out_shape=jax.ShapeDtypeStruct((few, width), bf16),
        in_specs=[here, here] + [away] * 6 + [here] + [away] * 3,
        out_specs=here,
        scratch_shapes=[
            vmem((8, few, width), bf16),
            vmem((width, heads * depth), bf16),
            vmem((width, 2 * depth), bf16),
            vmem((width, 3 * channels), bf16),
            vmem((channels + heads * depth, width), bf16),
            vmem(log_gate_cache.shape, f32),
            vmem((heads, 2 * ring * ring, block), f32),
            vmem((heads * span, depth), bf16),
            slots,
            slots,
            vmem((heads * span, 128), f32),
            vmem((heads * span, 128), f32),
            vmem((heads * span, depth), f32),
            vmem((16, channels), bf16),
            vmem((16, channels), bf16),
            vmem((span + 16, channels), f32),
            vmem((span, channels), bf16),
            vmem((span, channels + heads * depth), bf16),
            vmem((chunks, 4, few, columns), bf16),
            vmem((chunks, 4, few, columns), bf16),
            vmem((chunks, 4, few, columns), bf16),
            vmem((chunks, 4, few, columns), bf16),
            vmem((chunks, few, columns), bf16),
            vmem((chunks, few, columns), bf16),
            vmem((chunks, 2, few, columns), bf16),
            dma((9,)),
            dma((6,)),
            dma((6,)),
            dma((4,)),
            dma((4,)),
            dma((2,)),
            dma((ring,)),
            dma((ring, ring)),
            dma((ring, ring)),
            dma((ring, ring)),
            dma((ring, ring)),
            dma((ring, ring)),
            dma((chunks,)),
            dma((chunks,)),
            dma((chunks,)),
            dma((chunks,)),
            dma((chunks, 2)),
            dma((chunks, 2)),
        ],
        compiler_params=pltpu.CompilerParams(
            collective_id=0, has_side_effects=True, vmem_limit_bytes=60 << 20
        ),
        name="layer",
    )(
        tokens,
        norm_gain.reshape(1, width),
        w_query,
        w_key,
        w_value,
        w_conv_value,
        w_conv_pre,
        w_conv_post,
        conv_taps,
        log_gate_cache,
        w_out_conv,
        w_out_attn,
    )


def solution(mesh):
    placed = (
        P(("sp", "fs", "tp"), None),
        P(),
        P(None, ("fs", "tp")),
        P(None, "fs"),
        P(None, "fs"),
        P(None, ("fs", "tp")),
        P(None, ("fs", "tp")),
        P(None, ("fs", "tp")),
        P(),
        P(),
        P(("fs", "tp"), None),
        P(("fs", "tp"), None),
    )
    return jax.shard_map(
        shards, mesh=mesh, in_specs=placed, out_specs=P(("sp", "fs", "tp"), None), check_vma=False
    )
```

```python
import functools
import math

import jax
import jax.numpy as jnp
from jax import lax
from jax.experimental import pallas as pl
from jax.experimental.pallas import tpu as pltpu
from jax.sharding import PartitionSpec as P

epsilon = 1e-06
masked_score = -1e30
MESH = pl.DeviceIdType.MESH
log2_e = math.log2(math.e)


def arrival_order(ring):
    half = ring // 2
    pieces = []
    for slot in range(ring):
        hops = slot if slot <= half else slot - half
        for j in range(ring):
            pieces.append((hops + (j + 1) // 2, hops, slot, j))
    return [(slot, j) for _, _, slot, j in sorted(pieces)]


def chosen(values, t):
    if isinstance(t, int):
        return values[t]
    words = [values[n : n + 8] for n in range(0, len(values), 8)]
    packed = [sum(v << (3 * n) for n, v in enumerate(word)) for word in words]
    picked = jnp.int32(packed[-1])
    for n in range(len(packed) - 2, -1, -1):
        picked = jnp.where(t < 8 * (n + 1), jnp.int32(packed[n]), picked)
    return (picked >> (3 * (t % 8))) & 7


def layer_kernel(
    ring,
    tokens,
    gain,
    w_query,
    w_key,
    w_value,
    w_conv_value,
    w_conv_pre,
    w_conv_post,
    taps,
    log_gates,
    w_out_conv,
    w_out_attn,
    out_ref,
    rows,
    wq,
    wkv,
    wconv,
    wout,
    gates,
    bias_of,
    q_ref,
    own,
    other,
    row_max,
    row_sum,
    total,
    mixed_tail,
    halo,
    extended,
    gate_after,
    merged,
    part_keep,
    part_send,
    part_come,
    pair,
    relay,
    passed,
    come,
    weight_sem,
    gx_send,
    gx_recv,
    gd_send,
    gd_recv,
    halo_sem,
    s1,
    sr,
    sl,
    sd,
    r_own,
    r_other,
    pd_send,
    pd_recv,
    relay_send,
    relay_recv,
    come_send,
    come_recv,
):
    half = ring // 2
    group = ring // 2
    sp = lax.axis_index("sp")
    x = lax.axis_index("fs")
    core = lax.axis_index("tp")
    z, y = sp // ring, sp % ring
    far = 1 - core
    device = x * 2 + core
    blocks = ring * ring
    bf16 = jnp.bfloat16
    f32 = jnp.float32

    def first_axis(step):
        y1 = (y + far * step + ring) % ring
        z1 = (z + core * step + ring) % ring
        return {"sp": z1 * ring + y1}

    def second_axis(step):
        y1 = (y + core * step + ring) % ring
        z1 = (z + far * step + ring) % ring
        return {"sp": z1 * ring + y1}

    def along_x(step):
        return {"fs": (x + step + 4) % 4}

    partner = {"tp": far}
    after = {"sp": (sp + 1) % blocks}
    before = {"sp": (sp + blocks - 1) % blocks}

    def copy(src, dst, send, recv, who):
        return pltpu.make_async_remote_copy(
            src_ref=src, dst_ref=dst, send_sem=send, recv_sem=recv, device_id=who, device_id_type=MESH
        )

    depth = w_key.shape[1]
    channels = w_conv_post.shape[1]
    loads = [
        (log_gates, gates),
        (w_key, wkv.at[:, pl.ds(0, depth)]),
        (w_value, wkv.at[:, pl.ds(depth, depth)]),
        (w_query, wq),
        (w_conv_post, wconv.at[:, pl.ds(0, channels)]),
        (w_conv_pre, wconv.at[:, pl.ds(channels, channels)]),
        (w_conv_value, wconv.at[:, pl.ds(2 * channels, channels)]),
        (w_out_conv, wout.at[pl.ds(0, channels)]),
        (w_out_attn, wout.at[pl.ds(channels, 2 * depth)]),
    ]
    loads = [pltpu.make_async_copy(a, b, weight_sem.at[n]) for n, (a, b) in enumerate(loads)]
    for load in loads:
        load.start()

    barrier = pltpu.get_barrier_semaphore()
    near = (
        first_axis(1),
        first_axis(-1),
        second_axis(1),
        second_axis(-1),
        partner,
        along_x(1),
        along_x(-1),
        after,
        before,
    )
    for who in near:
        pl.semaphore_signal(barrier, inc=1, device_id=who, device_id_type=MESH)

    wide = tokens[...].astype(f32)
    scaled = wide * lax.rsqrt(jnp.mean(wide * wide, axis=1, keepdims=True) + epsilon)
    rows[device] = (scaled * gain[...]).astype(bf16)
    row_max[...] = jnp.full_like(row_max, masked_score)
    row_sum[...] = jnp.zeros_like(row_sum)
    total[...] = jnp.zeros_like(total)
    pl.semaphore_wait(barrier, len(near))

    few = rows.shape[1] // 2

    def of_x(step):
        return (x + step + 4) % 4 * 2 + core

    def piece_of(step, h):
        return rows.at[of_x(step), pl.ds(h * few, few)]

    def gather_x(step, h, sem, way):
        return copy(piece_of(step, h), piece_of(step, h), gx_send.at[sem], gx_recv.at[sem], along_x(way))

    def gather_across(step, n):
        here = rows.at[of_x(step)]
        return copy(here, here, gd_send.at[n], gd_recv.at[n], partner)

    def came_x(step, h, sem):
        return copy(piece_of(step, h), piece_of(step, h), gx_send.at[sem], gx_recv.at[sem], partner)

    first = [
        gather_x(0, 0, 0, 1),
        gather_x(0, 1, 1, -1),
        gather_x(0, 1, 2, 1),
        gather_x(0, 0, 3, -1),
    ]
    for one in first:
        one.start()
    crossing = [gather_across(0, 0)]
    crossing[0].start()

    heads = 2
    keys_of_block = bias_of.shape[2]
    loads[0].wait()
    row = lax.broadcasted_iota(jnp.int32, (gates.shape[0], keys_of_block), 0)
    for head in range(heads):
        mine = row == device * heads + head
        for n in range(0, bias_of.shape[1], 8):
            lines = [
                jnp.sum(
                    jnp.where(mine, gates[:, b * keys_of_block : (b + 1) * keys_of_block], 0.0),
                    axis=0,
                    keepdims=True,
                )
                for b in range(n, n + 8)
            ]
            seen = n + lax.broadcasted_iota(jnp.int32, (8, keys_of_block), 0) < 2 * sp + 2
            bias_of[head, n : n + 8] = jnp.where(
                seen, jnp.concatenate(lines, axis=0) * -log2_e, masked_score
            )

    came_x(-1, 0, 0).wait_recv()
    second = [gather_x(-1, 0, 4, 1)]
    second[0].start()
    came_x(1, 1, 1).wait_recv()
    second.append(gather_x(1, 1, 5, -1))
    second[1].start()
    came_x(-1, 1, 2).wait_recv()
    crossing.append(gather_across(-1, 1))
    crossing[1].start()
    came_x(1, 0, 3).wait_recv()
    crossing.append(gather_across(1, 2))
    crossing[2].start()
    came_x(2, 0, 4).wait_recv()
    came_x(2, 1, 5).wait_recv()
    crossing.append(gather_across(2, 3))
    crossing[3].start()
    for n in range(4):
        here = rows.at[(x + (0, -1, 1, 2)[n] + 4) % 4 * 2 + far]
        copy(here, here, gd_send.at[n], gd_recv.at[n], partner).wait_recv()

    width = rows.shape[2]
    block = own.shape[3]
    loads[1].wait()
    loads[2].wait()
    half_rows = rows[pl.ds(4 * core, 4)].reshape(block, width)
    made = jnp.dot(half_rows, wkv[...], preferred_element_type=f32).astype(bf16)
    own[0, 0, 0] = made[:, :depth]
    own[0, 0, 1] = made[:, depth:]

    def along(src, j, step):
        return copy(src, own.at[0, j], s1.at[j], r_own.at[0, j], first_axis(step))

    def right(src, slot, j):
        return copy(src, own.at[slot, j], sr.at[slot, j], r_own.at[slot, j], second_axis(1))

    def left(src, slot, j):
        return copy(src, own.at[slot, j], sl.at[slot, j], r_own.at[slot, j], second_axis(-1))

    def across(src, slot, j):
        return copy(src, other.at[slot, j], sd.at[slot, j], r_other.at[slot, j], partner)

    def arrived(slot, j):
        copy(own.at[slot, j], own.at[slot, j], sd.at[slot, j], r_own.at[slot, j], partner).wait_recv()

    def arrived_other(slot, j):
        copy(other.at[slot, j], other.at[slot, j], sd.at[slot, j], r_other.at[slot, j], partner).wait_recv()

    here = own.at[0, 0]
    along(here, 1, 1).start()
    along(here, 2, -1).start()
    right(here, 1, 0).start()
    left(here, half + 1, 0).start()
    across(here, 0, 0).start()

    span = rows.shape[0] * rows.shape[1]
    all_rows = rows[...].reshape(span, width)
    loads[3].wait()
    asked = jnp.dot(all_rows, wq[...], preferred_element_type=f32).astype(bf16)
    for head in range(heads):
        q_ref[pl.ds(head * span, span), :] = asked[:, head * depth : (head + 1) * depth]
    for n in (4, 5, 6):
        loads[n].wait()
    projected = jnp.dot(all_rows, wconv[...], preferred_element_type=f32).astype(bf16)
    gate_after[...] = projected[:, :channels]
    mixed_in = (
        projected[:, channels : 2 * channels].astype(f32) * projected[:, 2 * channels :].astype(f32)
    ).astype(bf16)
    edge = halo.shape[0]
    mixed_tail[...] = mixed_in[span - edge :]
    extended[pl.ds(edge, span), :] = mixed_in.astype(f32)
    shift = copy(mixed_tail, halo, halo_sem.at[0], halo_sem.at[1], after)
    shift.start()
    factor = depth ** (-0.5) * log2_e

    def place(slot, j, origin):
        dp = slot - (slot // (half + 1)) * (2 * slot - half)
        ds = (j + 1) // 2 * (2 * (j % 2) - 1)
        z1 = (z - dp + origin * (dp - ds) + 2 * ring) % ring
        y1 = (y - ds + origin * (ds - dp) + 2 * ring) % ring
        return z1 * ring + y1

    def attend(parts, pieces, diagonal=False):
        blocks_of = [(buffer, slot, j, origin) for buffer, origin in parts for slot, j in pieces]

        def score_of(unit):
            head, some = unit
            keys = jnp.concatenate([buffer[slot, j, 0] for buffer, slot, j, _ in some], axis=0)
            return lax.dot_general(
                q_ref[pl.ds(head * span, span), :],
                keys,
                (((1,), (1,)), ((), ())),
                preferred_element_type=f32,
            )

        def absorb(score, unit):
            head, some = unit
            here = pl.ds(head * span, span)
            values = jnp.concatenate([buffer[slot, j, 1] for buffer, slot, j, _ in some], axis=0)
            parts_of = []
            for n, (_, slot, j, origin) in enumerate(some):
                bias = bias_of[head, pl.ds(place(slot, j, origin) * 2 + origin, 1), :]
                part = score[:, n * block : (n + 1) * block] * factor + bias
                if diagonal and slot == 0 and j == 0:
                    at = lax.broadcasted_iota(jnp.int32, part.shape, 0)
                    key = lax.broadcasted_iota(jnp.int32, part.shape, 1)
                    part = jnp.where(key + origin * block > at, masked_score, part)
                parts_of.append(part)
            top = parts_of[0]
            for part in parts_of[1:]:
                top = jnp.maximum(top, part)
            old = row_max[here, :]
            new = jnp.maximum(old, jnp.max(top, axis=1, keepdims=True))
            rescale = jnp.exp2(old - new)
            weights = [jnp.exp2(part - new) for part in parts_of]
            lanes = weights[0]
            for weight in weights[1:]:
                lanes = lanes + weight
            row_max[here, :] = new
            row_sum[here, :] = row_sum[here, :] * rescale + lanes
            weight = jnp.concatenate([weight.astype(bf16) for weight in weights], axis=1)
            total[here, :] = total[here, :] * rescale + jnp.dot(
                weight, values, preferred_element_type=f32
            )

        units = [(head, blocks_of) for head in range(heads)]
        ahead = [score_of(unit) for unit in units[:1]]
        for n, unit in enumerate(units):
            if n + 1 < len(units):
                ahead.append(score_of(units[n + 1]))
            absorb(ahead[n], unit)

    order = arrival_order(ring)
    turns = len(order) // group

    def at_turn(t, i):
        slots = [order[n * group + i][0] for n in range(turns)]
        places = [order[n * group + i][1] for n in range(turns)]
        return chosen(slots, t), chosen(places, t)

    def pass_on(t):
        for i in range(group):
            slot, j = at_turn(t, i)
            here = own.at[slot, j]
            arrived(slot, j)
            odd = j % 2

            @pl.when((slot == 0) & (j + 2 < ring))
            def _():
                along(here, j + 2, 2 * odd - 1).start()

            @pl.when((slot < half - 1) | ((slot == half - 1) & (odd == 1)))
            def _():
                right(here, slot + 1, j).start()

            down = jnp.where(slot == 0, half, slot)

            @pl.when((slot == 0) | ((slot > half) & ((slot < ring - 1) | (odd == 0))))
            def _():
                left(here, jnp.where(slot == ring - 1, half, down + 1), j).start()

            across(here, slot, j).start()

    def attend_turn(t, diagonal=False):
        pieces = [at_turn(t, i) for i in range(group)]
        for slot, j in pieces:
            arrived_other(slot, j)
        attend(((own, core), (other, far)), pieces, diagonal)

    for i in range(1, group):
        slot, j = order[i]
        here = own.at[slot, j]
        arrived(slot, j)
        if slot == 0:
            along(here, j + 2, 2 * (j % 2) - 1).start()
            left(here, half + 1, j).start()
        if slot > half:
            left(here, slot + 1, j).start()
        else:
            right(here, slot + 1, j).start()
        across(here, slot, j).start()
    pass_on(jnp.int32(1))
    attend_turn(0, diagonal=True)

    def turn(t, carry):
        pass_on(t)
        attend_turn(t - 1)
        return carry

    lax.fori_loop(2, turns, turn, 0)

    shift.wait()
    extended[pl.ds(0, edge), :] = jnp.where(sp == 0, 0.0, halo[...].astype(f32))
    at = pl.multiple_of(device * channels, channels)
    tap_rows = taps[:, pl.ds(at, channels)].astype(f32)
    count = tap_rows.shape[0]
    conv_sum = tap_rows[0:1] * extended[pl.ds(edge - count + 1, span), :]
    for n in range(1, count):
        conv_sum = conv_sum + tap_rows[n : n + 1] * extended[pl.ds(edge - count + 1 + n, span), :]
    merged[:, pl.ds(0, channels)] = (gate_after[...].astype(f32) * conv_sum).astype(bf16)

    attend_turn(turns - 1)
    for head in range(heads):
        here = pl.ds(head * span, span)
        merged[:, pl.ds(channels + head * depth, depth)] = (
            total[here, :] / jnp.sum(row_sum[here, :], axis=1, keepdims=True)
        ).astype(bf16)

    loads[7].wait()
    loads[8].wait()
    chunks = part_keep.shape[0]
    columns = part_keep.shape[3]

    def to_partner(k):
        return copy(part_send.at[k], part_come.at[k], pd_send.at[k], pd_recv.at[k], partner)

    def way(k):
        return 1 if k % 2 == 0 else -1

    def to_relay(k):
        return copy(pair.at[k, (x + 2) % 4], relay.at[k], relay_send.at[k], relay_recv.at[k], along_x(way(k)))

    def straight(k):
        return copy(
            pair.at[k, (x - way(k) + 4) % 4],
            come.at[k, 1],
            come_send.at[k, 1],
            come_recv.at[k, 1],
            along_x(-way(k)),
        )

    def relayed(k):
        return copy(passed.at[k], come.at[k, 0], come_send.at[k, 0], come_recv.at[k, 0], along_x(way(k)))

    def project(k):
        part = jnp.dot(
            merged[...], wout[:, pl.ds(k * columns, columns)], preferred_element_type=f32
        ).astype(bf16)
        part = part.reshape(4, 2, span // 8, columns)
        part_send[k] = jnp.where(core == 0, part[:, 1], part[:, 0])
        part_keep[k] = jnp.where(core == 0, part[:, 0], part[:, 1])
        to_partner(k).start()

    def add_pair(k):
        to_partner(k).wait_recv()
        pair[k] = (part_keep[k].astype(f32) + part_come[k].astype(f32)).astype(bf16)
        to_relay(k).start()
        straight(k).start()

    def add_relay(k):
        to_relay(k).wait_recv()
        mine = pair[k, (x + way(k) + 4) % 4].astype(f32)
        passed[k] = (mine + relay[k].astype(f32)).astype(bf16)
        relayed(k).start()

    def finish(k):
        straight(k).wait_recv()
        relayed(k).wait_recv()
        out_ref[:, pl.ds(k * columns, columns)] = (
            pair[k, x].astype(f32) + come[k, 0].astype(f32) + come[k, 1].astype(f32)
        ).astype(out_ref.dtype)

    for k in range(chunks + 1):
        if k < chunks:
            project(k)
        if k > 0:
            add_pair(k - 1)
    for k in range(chunks):
        add_relay(k)
    for k in range(chunks):
        finish(k)

    for one in first + second + crossing:
        one.wait_send()
    for k in range(chunks):
        to_partner(k).wait_send()
        to_relay(k).wait_send()
        straight(k).wait_send()
        relayed(k).wait_send()
    for j in range(1, ring):
        along(own.at[0, j], j, 1).wait_send()

    def sent(j, carry):
        for slot in range(1, half):
            right(own.at[slot, j], slot, j).wait_send()
            left(own.at[half + slot, j], half + slot, j).wait_send()
        for slot in range(ring):
            across(own.at[slot, j], slot, j).wait_send()
        return carry

    lax.fori_loop(0, ring, sent, 0)

    def sent_far(t, carry):
        right(own.at[half, 2 * t + 1], half, 2 * t + 1).wait_send()
        left(own.at[half, 2 * t], half, 2 * t).wait_send()
        return carry

    lax.fori_loop(0, half, sent_far, 0)


def shards(
    tokens,
    norm_gain,
    w_query,
    w_key,
    w_value,
    w_conv_value,
    w_conv_pre,
    w_conv_post,
    conv_taps,
    log_gate_cache,
    w_out_conv,
    w_out_attn,
):
    ring = math.isqrt(lax.axis_size("sp"))
    few, width = tokens.shape
    span = 8 * few
    depth = w_key.shape[1]
    channels = w_conv_post.shape[1]
    heads = w_query.shape[1] // depth
    block = span // 2
    chunks = 4
    columns = width // chunks
    bf16, f32 = jnp.bfloat16, jnp.float32
    dma = pltpu.SemaphoreType.DMA
    vmem = pltpu.VMEM
    here = pl.BlockSpec(memory_space=pltpu.VMEM)
    away = pl.BlockSpec(memory_space=pl.ANY)
    slots = vmem((ring, ring, 2, block, depth), bf16)
    return pl.pallas_call(
        functools.partial(layer_kernel, ring),
        out_shape=jax.ShapeDtypeStruct((few, width), bf16),
        in_specs=[here, here] + [away] * 6 + [here] + [away] * 3,
        out_specs=here,
        scratch_shapes=[
            vmem((8, few, width), bf16),
            vmem((width, heads * depth), bf16),
            vmem((width, 2 * depth), bf16),
            vmem((width, 3 * channels), bf16),
            vmem((channels + heads * depth, width), bf16),
            vmem(log_gate_cache.shape, f32),
            vmem((heads, 2 * ring * ring, block), f32),
            vmem((heads * span, depth), bf16),
            slots,
            slots,
            vmem((heads * span, 128), f32),
            vmem((heads * span, 128), f32),
            vmem((heads * span, depth), f32),
            vmem((16, channels), bf16),
            vmem((16, channels), bf16),
            vmem((span + 16, channels), f32),
            vmem((span, channels), bf16),
            vmem((span, channels + heads * depth), bf16),
            vmem((chunks, 4, few, columns), bf16),
            vmem((chunks, 4, few, columns), bf16),
            vmem((chunks, 4, few, columns), bf16),
            vmem((chunks, 4, few, columns), bf16),
            vmem((chunks, few, columns), bf16),
            vmem((chunks, few, columns), bf16),
            vmem((chunks, 2, few, columns), bf16),
            dma((9,)),
            dma((6,)),
            dma((6,)),
            dma((4,)),
            dma((4,)),
            dma((2,)),
            dma((ring,)),
            dma((ring, ring)),
            dma((ring, ring)),
            dma((ring, ring)),
            dma((ring, ring)),
            dma((ring, ring)),
            dma((chunks,)),
            dma((chunks,)),
            dma((chunks,)),
            dma((chunks,)),
            dma((chunks, 2)),
            dma((chunks, 2)),
        ],
        compiler_params=pltpu.CompilerParams(
            collective_id=0, has_side_effects=True, vmem_limit_bytes=60 << 20
        ),
        name="layer",
    )(
        tokens,
        norm_gain.reshape(1, width),
        w_query,
        w_key,
        w_value,
        w_conv_value,
        w_conv_pre,
        w_conv_post,
        conv_taps,
        log_gate_cache,
        w_out_conv,
        w_out_attn,
    )


def solution(mesh):
    placed = (
        P(("sp", "fs", "tp"), None),
        P(),
        P(None, ("fs", "tp")),
        P(None, "fs"),
        P(None, "fs"),
        P(None, ("fs", "tp")),
        P(None, ("fs", "tp")),
        P(None, ("fs", "tp")),
        P(),
        P(),
        P(("fs", "tp"), None),
        P(("fs", "tp"), None),
    )
    return jax.shard_map(
        shards, mesh=mesh, in_specs=placed, out_specs=P(("sp", "fs", "tp"), None), check_vma=False
    )
```

```python
import functools
import math

import jax
import jax.numpy as jnp
from jax import lax
from jax.experimental import pallas as pl
from jax.experimental.pallas import tpu as pltpu
from jax.sharding import PartitionSpec as P

epsilon = 1e-06
masked_score = -1e30
MESH = pl.DeviceIdType.MESH
log2_e = math.log2(math.e)


def arrival_order(ring):
    half = ring // 2
    pieces = []
    for slot in range(ring):
        hops = slot if slot <= half else slot - half
        for j in range(ring):
            pieces.append((10 * hops + 8 * ((j + 1) // 2), hops, slot, j))
    return [(slot, j) for _, _, slot, j in sorted(pieces)]


def chosen(values, t):
    if isinstance(t, int):
        return values[t]
    words = [values[n : n + 8] for n in range(0, len(values), 8)]
    packed = [sum(v << (3 * n) for n, v in enumerate(word)) for word in words]
    picked = jnp.int32(packed[-1])
    for n in range(len(packed) - 2, -1, -1):
        picked = jnp.where(t < 8 * (n + 1), jnp.int32(packed[n]), picked)
    return (picked >> (3 * (t % 8))) & 7


def layer_kernel(
    ring,
    tokens,
    gain,
    w_query,
    w_key,
    w_value,
    w_conv_value,
    w_conv_pre,
    w_conv_post,
    taps,
    log_gates,
    w_out_conv,
    w_out_attn,
    out_ref,
    rows,
    wq,
    wkv,
    wconv,
    wout,
    gates,
    bias_of,
    q_ref,
    own,
    other,
    row_max,
    row_sum,
    total,
    mixed_tail,
    halo,
    extended,
    gate_after,
    merged,
    part_keep,
    part_send,
    part_come,
    pair,
    relay,
    passed,
    come,
    weight_sem,
    gx_send,
    gx_recv,
    gd_send,
    gd_recv,
    halo_sem,
    s1,
    sr,
    sl,
    sd,
    r_own,
    r_other,
    pd_send,
    pd_recv,
    relay_send,
    relay_recv,
    come_send,
    come_recv,
):
    half = ring // 2
    group = ring // 2
    sp = lax.axis_index("sp")
    x = lax.axis_index("fs")
    core = lax.axis_index("tp")
    z, y = sp // ring, sp % ring
    far = 1 - core
    device = x * 2 + core
    blocks = ring * ring
    bf16 = jnp.bfloat16
    f32 = jnp.float32

    def first_axis(step):
        y1 = (y + far * step + ring) % ring
        z1 = (z + core * step + ring) % ring
        return {"sp": z1 * ring + y1}

    def second_axis(step):
        y1 = (y + core * step + ring) % ring
        z1 = (z + far * step + ring) % ring
        return {"sp": z1 * ring + y1}

    def along_x(step):
        return {"fs": (x + step + 4) % 4}

    partner = {"tp": far}
    after = {"sp": (sp + 1) % blocks}
    before = {"sp": (sp + blocks - 1) % blocks}

    def copy(src, dst, send, recv, who):
        return pltpu.make_async_remote_copy(
            src_ref=src, dst_ref=dst, send_sem=send, recv_sem=recv, device_id=who, device_id_type=MESH
        )

    depth = w_key.shape[1]
    channels = w_conv_post.shape[1]
    loads = [
        (log_gates, gates),
        (w_key, wkv.at[:, pl.ds(0, depth)]),
        (w_value, wkv.at[:, pl.ds(depth, depth)]),
        (w_query, wq),
        (w_conv_post, wconv.at[:, pl.ds(0, channels)]),
        (w_conv_pre, wconv.at[:, pl.ds(channels, channels)]),
        (w_conv_value, wconv.at[:, pl.ds(2 * channels, channels)]),
        (w_out_conv, wout.at[pl.ds(0, channels)]),
        (w_out_attn, wout.at[pl.ds(channels, 2 * depth)]),
    ]
    loads = [pltpu.make_async_copy(a, b, weight_sem.at[n]) for n, (a, b) in enumerate(loads)]
    for load in loads:
        load.start()

    barrier = pltpu.get_barrier_semaphore()
    near = (
        first_axis(1),
        first_axis(-1),
        second_axis(1),
        second_axis(-1),
        partner,
        along_x(1),
        along_x(-1),
        after,
        before,
    )
    for who in near:
        pl.semaphore_signal(barrier, inc=1, device_id=who, device_id_type=MESH)

    wide = tokens[...].astype(f32)
    scaled = wide * lax.rsqrt(jnp.mean(wide * wide, axis=1, keepdims=True) + epsilon)
    rows[device] = (scaled * gain[...]).astype(bf16)
    row_max[...] = jnp.full_like(row_max, masked_score)
    row_sum[...] = jnp.zeros_like(row_sum)
    total[...] = jnp.zeros_like(total)
    pl.semaphore_wait(barrier, len(near))

    few = rows.shape[1] // 2

    def of_x(step):
        return (x + step + 4) % 4 * 2 + core

    def piece_of(step, h):
        return rows.at[of_x(step), pl.ds(h * few, few)]

    def gather_x(step, h, sem, way):
        return copy(piece_of(step, h), piece_of(step, h), gx_send.at[sem], gx_recv.at[sem], along_x(way))

    def gather_across(step, n):
        here = rows.at[of_x(step)]
        return copy(here, here, gd_send.at[n], gd_recv.at[n], partner)

    def came_x(step, h, sem):
        return copy(piece_of(step, h), piece_of(step, h), gx_send.at[sem], gx_recv.at[sem], partner)

    first = [
        gather_x(0, 0, 0, 1),
        gather_x(0, 1, 1, -1),
        gather_x(0, 1, 2, 1),
        gather_x(0, 0, 3, -1),
    ]
    for one in first:
        one.start()
    crossing = [gather_across(0, 0)]
    crossing[0].start()

    heads = 2
    keys_of_block = bias_of.shape[2]
    loads[0].wait()
    row = lax.broadcasted_iota(jnp.int32, (gates.shape[0], keys_of_block), 0)
    for head in range(heads):
        mine = row == device * heads + head
        for n in range(0, bias_of.shape[1], 8):
            lines = [
                jnp.sum(
                    jnp.where(mine, gates[:, b * keys_of_block : (b + 1) * keys_of_block], 0.0),
                    axis=0,
                    keepdims=True,
                )
                for b in range(n, n + 8)
            ]
            seen = n + lax.broadcasted_iota(jnp.int32, (8, keys_of_block), 0) < 2 * sp + 2
            bias_of[head, n : n + 8] = jnp.where(
                seen, jnp.concatenate(lines, axis=0) * -log2_e, masked_score
            )

    came_x(-1, 0, 0).wait_recv()
    second = [gather_x(-1, 0, 4, 1)]
    second[0].start()
    came_x(1, 1, 1).wait_recv()
    second.append(gather_x(1, 1, 5, -1))
    second[1].start()
    came_x(-1, 1, 2).wait_recv()
    crossing.append(gather_across(-1, 1))
    crossing[1].start()
    came_x(1, 0, 3).wait_recv()
    crossing.append(gather_across(1, 2))
    crossing[2].start()
    came_x(2, 0, 4).wait_recv()
    came_x(2, 1, 5).wait_recv()
    crossing.append(gather_across(2, 3))
    crossing[3].start()
    for n in range(4):
        here = rows.at[(x + (0, -1, 1, 2)[n] + 4) % 4 * 2 + far]
        copy(here, here, gd_send.at[n], gd_recv.at[n], partner).wait_recv()

    width = rows.shape[2]
    block = own.shape[3]
    loads[1].wait()
    loads[2].wait()
    half_rows = rows[pl.ds(4 * core, 4)].reshape(block, width)
    made = jnp.dot(half_rows, wkv[...], preferred_element_type=f32).astype(bf16)
    own[0, 0, 0] = made[:, :depth]
    own[0, 0, 1] = made[:, depth:]

    def along(src, j, step):
        return copy(src, own.at[0, j], s1.at[j], r_own.at[0, j], first_axis(step))

    def right(src, slot, j):
        return copy(src, own.at[slot, j], sr.at[slot, j], r_own.at[slot, j], second_axis(1))

    def left(src, slot, j):
        return copy(src, own.at[slot, j], sl.at[slot, j], r_own.at[slot, j], second_axis(-1))

    def across(src, slot, j):
        return copy(src, other.at[slot, j], sd.at[slot, j], r_other.at[slot, j], partner)

    def arrived(slot, j):
        copy(own.at[slot, j], own.at[slot, j], sd.at[slot, j], r_own.at[slot, j], partner).wait_recv()

    def arrived_other(slot, j):
        copy(other.at[slot, j], other.at[slot, j], sd.at[slot, j], r_other.at[slot, j], partner).wait_recv()

    here = own.at[0, 0]
    along(here, 1, 1).start()
    along(here, 2, -1).start()
    right(here, 1, 0).start()
    left(here, half + 1, 0).start()
    across(here, 0, 0).start()

    span = rows.shape[0] * rows.shape[1]
    all_rows = rows[...].reshape(span, width)
    loads[3].wait()
    asked = jnp.dot(all_rows, wq[...], preferred_element_type=f32).astype(bf16)
    for head in range(heads):
        q_ref[pl.ds(head * span, span), :] = asked[:, head * depth : (head + 1) * depth]
    for n in (4, 5, 6):
        loads[n].wait()
    projected = jnp.dot(all_rows, wconv[...], preferred_element_type=f32).astype(bf16)
    gate_after[...] = projected[:, :channels]
    mixed_in = (
        projected[:, channels : 2 * channels].astype(f32) * projected[:, 2 * channels :].astype(f32)
    ).astype(bf16)
    edge = halo.shape[0]
    mixed_tail[...] = mixed_in[span - edge :]
    extended[pl.ds(edge, span), :] = mixed_in.astype(f32)
    shift = copy(mixed_tail, halo, halo_sem.at[0], halo_sem.at[1], after)
    shift.start()
    factor = depth ** (-0.5) * log2_e

    def place(slot, j, origin):
        dp = slot - (slot // (half + 1)) * (2 * slot - half)
        ds = (j + 1) // 2 * (2 * (j % 2) - 1)
        z1 = (z - dp + origin * (dp - ds) + 2 * ring) % ring
        y1 = (y - ds + origin * (ds - dp) + 2 * ring) % ring
        return z1 * ring + y1

    def attend(parts, pieces, diagonal=False):
        blocks_of = [(buffer, slot, j, origin) for buffer, origin in parts for slot, j in pieces]

        def score_of(unit):
            head, some = unit
            keys = jnp.concatenate([buffer[slot, j, 0] for buffer, slot, j, _ in some], axis=0)
            return lax.dot_general(
                q_ref[pl.ds(head * span, span), :],
                keys,
                (((1,), (1,)), ((), ())),
                preferred_element_type=f32,
            )

        def absorb(score, unit):
            head, some = unit
            here = pl.ds(head * span, span)
            values = jnp.concatenate([buffer[slot, j, 1] for buffer, slot, j, _ in some], axis=0)
            parts_of = []
            for n, (_, slot, j, origin) in enumerate(some):
                bias = bias_of[head, pl.ds(place(slot, j, origin) * 2 + origin, 1), :]
                part = score[:, n * block : (n + 1) * block] * factor + bias
                if diagonal and slot == 0 and j == 0:
                    at = lax.broadcasted_iota(jnp.int32, part.shape, 0)
                    key = lax.broadcasted_iota(jnp.int32, part.shape, 1)
                    part = jnp.where(key + origin * block > at, masked_score, part)
                parts_of.append(part)
            top = parts_of[0]
            for part in parts_of[1:]:
                top = jnp.maximum(top, part)
            old = row_max[here, :]
            new = jnp.maximum(old, jnp.max(top, axis=1, keepdims=True))
            rescale = jnp.exp2(old - new)
            weights = [jnp.exp2(part - new) for part in parts_of]
            lanes = weights[0]
            for weight in weights[1:]:
                lanes = lanes + weight
            row_max[here, :] = new
            row_sum[here, :] = row_sum[here, :] * rescale + lanes
            weight = jnp.concatenate([weight.astype(bf16) for weight in weights], axis=1)
            total[here, :] = total[here, :] * rescale + jnp.dot(
                weight, values, preferred_element_type=f32
            )

        units = [(head, blocks_of) for head in range(heads)]
        ahead = [score_of(unit) for unit in units[:1]]
        for n, unit in enumerate(units):
            if n + 1 < len(units):
                ahead.append(score_of(units[n + 1]))
            absorb(ahead[n], unit)

    order = arrival_order(ring)
    turns = len(order) // group

    def at_turn(t, i):
        slots = [order[n * group + i][0] for n in range(turns)]
        places = [order[n * group + i][1] for n in range(turns)]
        return chosen(slots, t), chosen(places, t)

    def pass_on(t):
        for i in range(group):
            slot, j = at_turn(t, i)
            here = own.at[slot, j]
            arrived(slot, j)
            odd = j % 2

            @pl.when((slot == 0) & (j + 2 < ring))
            def _():
                along(here, j + 2, 2 * odd - 1).start()

            @pl.when((slot < half - 1) | ((slot == half - 1) & (odd == 1)))
            def _():
                right(here, slot + 1, j).start()

            down = jnp.where(slot == 0, half, slot)

            @pl.when((slot == 0) | ((slot > half) & ((slot < ring - 1) | (odd == 0))))
            def _():
                left(here, jnp.where(slot == ring - 1, half, down + 1), j).start()

            across(here, slot, j).start()

    def attend_turn(t, diagonal=False):
        pieces = [at_turn(t, i) for i in range(group)]
        for slot, j in pieces:
            arrived_other(slot, j)
        attend(((own, core), (other, far)), pieces, diagonal)

    for i in range(1, group):
        slot, j = order[i]
        here = own.at[slot, j]
        arrived(slot, j)
        if slot == 0:
            along(here, j + 2, 2 * (j % 2) - 1).start()
            left(here, half + 1, j).start()
        if slot > half:
            left(here, slot + 1, j).start()
        else:
            right(here, slot + 1, j).start()
        across(here, slot, j).start()
    pass_on(jnp.int32(1))
    shift.wait()
    extended[pl.ds(0, edge), :] = jnp.where(sp == 0, 0.0, halo[...].astype(f32))
    at = pl.multiple_of(device * channels, channels)
    tap_rows = taps[:, pl.ds(at, channels)].astype(f32)
    count = tap_rows.shape[0]
    conv_sum = tap_rows[0:1] * extended[pl.ds(edge - count + 1, span), :]
    for n in range(1, count):
        conv_sum = conv_sum + tap_rows[n : n + 1] * extended[pl.ds(edge - count + 1 + n, span), :]
    merged[:, pl.ds(0, channels)] = (gate_after[...].astype(f32) * conv_sum).astype(bf16)

    attend_turn(0, diagonal=True)

    def turn(t, carry):
        pass_on(t)
        attend_turn(t - 1)
        return carry

    lax.fori_loop(2, turns, turn, 0)

    attend_turn(turns - 1)
    for head in range(heads):
        here = pl.ds(head * span, span)
        merged[:, pl.ds(channels + head * depth, depth)] = (
            total[here, :] / jnp.sum(row_sum[here, :], axis=1, keepdims=True)
        ).astype(bf16)

    loads[7].wait()
    loads[8].wait()
    chunks = part_keep.shape[0]
    columns = part_keep.shape[3]

    def to_partner(k):
        return copy(part_send.at[k], part_come.at[k], pd_send.at[k], pd_recv.at[k], partner)

    def way(k):
        return 1 if k % 2 == 0 else -1

    def to_relay(k):
        return copy(pair.at[k, (x + 2) % 4], relay.at[k], relay_send.at[k], relay_recv.at[k], along_x(way(k)))

    def straight(k):
        return copy(
            pair.at[k, (x - way(k) + 4) % 4],
            come.at[k, 1],
            come_send.at[k, 1],
            come_recv.at[k, 1],
            along_x(-way(k)),
        )

    def relayed(k):
        return copy(passed.at[k], come.at[k, 0], come_send.at[k, 0], come_recv.at[k, 0], along_x(way(k)))

    def project(k):
        part = jnp.dot(
            merged[...], wout[:, pl.ds(k * columns, columns)], preferred_element_type=f32
        ).astype(bf16)
        part = part.reshape(4, 2, span // 8, columns)
        part_send[k] = jnp.where(core == 0, part[:, 1], part[:, 0])
        part_keep[k] = jnp.where(core == 0, part[:, 0], part[:, 1])
        to_partner(k).start()

    def add_pair(k):
        to_partner(k).wait_recv()
        pair[k] = (part_keep[k].astype(f32) + part_come[k].astype(f32)).astype(bf16)
        to_relay(k).start()
        straight(k).start()

    def add_relay(k):
        to_relay(k).wait_recv()
        mine = pair[k, (x + way(k) + 4) % 4].astype(f32)
        passed[k] = (mine + relay[k].astype(f32)).astype(bf16)
        relayed(k).start()

    def finish(k):
        straight(k).wait_recv()
        relayed(k).wait_recv()
        out_ref[:, pl.ds(k * columns, columns)] = (
            pair[k, x].astype(f32) + come[k, 0].astype(f32) + come[k, 1].astype(f32)
        ).astype(out_ref.dtype)

    for k in range(chunks + 1):
        if k < chunks:
            project(k)
        if k > 0:
            add_pair(k - 1)
    for one in first + second + crossing:
        one.wait_send()
    for j in range(1, ring):
        along(own.at[0, j], j, 1).wait_send()

    def sent(j, carry):
        for slot in range(1, half):
            right(own.at[slot, j], slot, j).wait_send()
            left(own.at[half + slot, j], half + slot, j).wait_send()
        for slot in range(ring):
            across(own.at[slot, j], slot, j).wait_send()
        return carry

    lax.fori_loop(0, ring, sent, 0)

    def sent_far(t, carry):
        right(own.at[half, 2 * t + 1], half, 2 * t + 1).wait_send()
        left(own.at[half, 2 * t], half, 2 * t).wait_send()
        return carry

    lax.fori_loop(0, half, sent_far, 0)

    for k in range(chunks):
        add_relay(k)
    for k in range(chunks):
        finish(k)

    for k in range(chunks):
        to_partner(k).wait_send()
        to_relay(k).wait_send()
        straight(k).wait_send()
        relayed(k).wait_send()


def shards(
    tokens,
    norm_gain,
    w_query,
    w_key,
    w_value,
    w_conv_value,
    w_conv_pre,
    w_conv_post,
    conv_taps,
    log_gate_cache,
    w_out_conv,
    w_out_attn,
):
    ring = math.isqrt(lax.axis_size("sp"))
    few, width = tokens.shape
    span = 8 * few
    depth = w_key.shape[1]
    channels = w_conv_post.shape[1]
    heads = w_query.shape[1] // depth
    block = span // 2
    chunks = 4
    columns = width // chunks
    bf16, f32 = jnp.bfloat16, jnp.float32
    dma = pltpu.SemaphoreType.DMA
    vmem = pltpu.VMEM
    here = pl.BlockSpec(memory_space=pltpu.VMEM)
    away = pl.BlockSpec(memory_space=pl.ANY)
    slots = vmem((ring, ring, 2, block, depth), bf16)
    return pl.pallas_call(
        functools.partial(layer_kernel, ring),
        out_shape=jax.ShapeDtypeStruct((few, width), bf16),
        in_specs=[here, here] + [away] * 6 + [here] + [away] * 3,
        out_specs=here,
        scratch_shapes=[
            vmem((8, few, width), bf16),
            vmem((width, heads * depth), bf16),
            vmem((width, 2 * depth), bf16),
            vmem((width, 3 * channels), bf16),
            vmem((channels + heads * depth, width), bf16),
            vmem(log_gate_cache.shape, f32),
            vmem((heads, 2 * ring * ring, block), f32),
            vmem((heads * span, depth), bf16),
            slots,
            slots,
            vmem((heads * span, 128), f32),
            vmem((heads * span, 128), f32),
            vmem((heads * span, depth), f32),
            vmem((16, channels), bf16),
            vmem((16, channels), bf16),
            vmem((span + 16, channels), f32),
            vmem((span, channels), bf16),
            vmem((span, channels + heads * depth), bf16),
            vmem((chunks, 4, few, columns), bf16),
            vmem((chunks, 4, few, columns), bf16),
            vmem((chunks, 4, few, columns), bf16),
            vmem((chunks, 4, few, columns), bf16),
            vmem((chunks, few, columns), bf16),
            vmem((chunks, few, columns), bf16),
            vmem((chunks, 2, few, columns), bf16),
            dma((9,)),
            dma((6,)),
            dma((6,)),
            dma((4,)),
            dma((4,)),
            dma((2,)),
            dma((ring,)),
            dma((ring, ring)),
            dma((ring, ring)),
            dma((ring, ring)),
            dma((ring, ring)),
            dma((ring, ring)),
            dma((chunks,)),
            dma((chunks,)),
            dma((chunks,)),
            dma((chunks,)),
            dma((chunks, 2)),
            dma((chunks, 2)),
        ],
        compiler_params=pltpu.CompilerParams(
            collective_id=0, has_side_effects=True, vmem_limit_bytes=60 << 20
        ),
        name="layer",
    )(
        tokens,
        norm_gain.reshape(1, width),
        w_query,
        w_key,
        w_value,
        w_conv_value,
        w_conv_pre,
        w_conv_post,
        conv_taps,
        log_gate_cache,
        w_out_conv,
        w_out_attn,
    )


def solution(mesh):
    placed = (
        P(("sp", "fs", "tp"), None),
        P(),
        P(None, ("fs", "tp")),
        P(None, "fs"),
        P(None, "fs"),
        P(None, ("fs", "tp")),
        P(None, ("fs", "tp")),
        P(None, ("fs", "tp")),
        P(),
        P(),
        P(("fs", "tp"), None),
        P(("fs", "tp"), None),
    )
    return jax.shard_map(
        shards, mesh=mesh, in_specs=placed, out_specs=P(("sp", "fs", "tp"), None), check_vma=False
    )
```
